32 devices in a mesh: sp: 8 (over z, x), dp: 4 (over y, core).
Axes of the slice: x: 2, y: 2, z: 4, core: 2. Of those that a mesh axis runs over, the one named last changes fastest.
Arguments:
- skip_stream_entering: bfloat16 [4, 1024, 2048], P('dp', 'sp'), may hold values from -6 to 6
- mapped_probe_matrix: bfloat16 [4, 1024, 2048], P('dp', 'sp'), may hold values from -6 to 6
- mapped_lookup_matrix: bfloat16 [4, 1024, 2048], P('dp', 'sp'), may hold values from -6 to 6
- mapped_content_matrix: bfloat16 [4, 1024, 4096], P('dp', 'sp'), may hold values from -6 to 6
- retention_preactivation: bfloat16 [4, 1024, 2048], P('dp', 'sp'), may hold values from -4 to 12
- extra_shrinkage: float32 [4, 16, 1024], P('dp', 'sp'), may hold values from -0.6932 to 0
- attention_group_scale: float32 [4096], replicated, may hold values from 0.1 to 1.9
- final_projection_matrix: bfloat16 [4096, 2048], P(None, 'dp'), may hold values from -0.09375 to 0.09375
- blender_branch_scale: float32 [2048], replicated, may hold values from 0.1 to 1.9
- specialist_prenormal_scale: float32 [2048], replicated, may hold values from 0.1 to 1.9
- specialist_switch_matrix: bfloat16 [32, 2048, 1024], P(('sp', 'dp')), may hold values from -0.125 to 0.125
- specialist_expand_matrix: bfloat16 [32, 2048, 1024], P(('sp', 'dp')), may hold values from -0.125 to 0.125
- specialist_contract_matrix: bfloat16 [32, 1024, 2048], P(('sp', 'dp')), may hold values from -0.1875 to 0.1875
- specialist_branch_scale: float32 [2048], replicated, may hold values from 0.1 to 1.9
- assigned_specialists: int32 [4, 1024, 2], P('dp', 'sp'), may hold values from 0 to 31, all different within a row; in each aligned block of 128 rows (0 to 127, 128 to 255, ..., all dimensions but the last counted through in order) at most 13 rows name the same one
- dispatcher_logits: float32 [4, 1024, 2], P('dp', 'sp'), may hold values from 0.2 to 1
Outputs:
- layer_out: bfloat16 [4, 1024, 2048], P('dp', 'sp')
The draws below stay inside these ranges and needn't reach their ends.
Inputs may be any that keep to these rules, and one draw needn't show every extreme that they name: `assigned_specialists`: in the rows of one device no expert is named more than 13 times; in every draw some expert reaches 13 on some device.
All inputs are finite; a program needn't handle non-finite values.
Results may differ from the reference program's by a relative error of at most 0.013.
Values may be sent and summed in bfloat16 or wider, within the bound.
A program may use at most 128 MiB of HBM per device.

```python
import math
import jax
import jax.numpy as jnp
import numpy as np
from jax import lax

D = 2048
ATTENTION_GROUPS = 16
KEY_WIDTH = 128
DV = 256
FF = 1024
TOP = 2
BLOCK = 64
TOK_DEV = 128
BATCH_SAMPLES = 4
TIME_STEPS = 1024
EXPERTS = 32
CAP = 13


def draw_retention_preactivation(key, part):
    kinds = jax.random.randint(jax.random.fold_in(key, 11), (ATTENTION_GROUPS,), 0, 10)
    slowness = (kinds >= 5).astype(jnp.float32)
    slow_center = math.log(TIME_STEPS / 24.0)
    centers = slowness * slow_center + (1.0 - slowness) * 0.5
    channel = jax.random.uniform(jax.random.fold_in(key, 12), (ATTENTION_GROUPS, KEY_WIDTH), jnp.float32, -0.5, 0.5)
    base_rate = (centers[:, None] + channel).reshape(ATTENTION_GROUPS * KEY_WIDTH)
    span_count = TIME_STEPS // TOK_DEV
    shifts = jax.random.uniform(jax.random.fold_in(key, 13), (BATCH_SAMPLES, span_count), jnp.float32, -0.7, 0.7)
    shifts = jnp.repeat(shifts, TOK_DEV, axis=1)
    jitter = 0.8 * jax.random.normal(jax.random.fold_in(key, 14), (BATCH_SAMPLES, TIME_STEPS, ATTENTION_GROUPS * KEY_WIDTH), jnp.float32)
    total = base_rate[None, None, :] + shifts[:, :, None] + jitter
    return jnp.clip(total, -4.0, 12.0).astype(jnp.bfloat16)


def draw_extra_shrinkage(key, part):
    spike_amount = 6
    timestep_offset = jax.random.randint(jax.random.fold_in(key, 21), (BATCH_SAMPLES, ATTENTION_GROUPS, spike_amount), 0, TIME_STEPS)
    tier_amount = jax.random.uniform(jax.random.fold_in(key, 22), (BATCH_SAMPLES, ATTENTION_GROUPS, spike_amount), jnp.float32, math.log(0.5), math.log(0.8))
    places = jnp.arange(TIME_STEPS, dtype=jnp.int32)
    matched = places[None, None, :, None] == timestep_offset[:, :, None, :]
    return jnp.min(jnp.where(matched, tier_amount[:, :, None, :], 0.0), axis=3)


def block_scale(key, dims, split, low, high):
    level = 1.0
    for dim, blocks in split:
        draws = jax.random.uniform(jax.random.fold_in(jax.random.fold_in(key, 6), dim), (blocks,), jnp.float32, low / len(split), high / len(split))
        level = level * jnp.repeat(jnp.exp(draws), dims[dim] // blocks).reshape((-1,) + (1,) * (len(dims) - 1 - dim))
    return level


def assign_block(stream_key, own, number, rows, number_of, top, bound, skew):
    order = jax.random.permutation(stream_key, number_of)
    packed, common = portions_of(number_of, rows * top, bound, skew, True), portions_of(number_of, rows * top, bound, skew, False)
    places = jnp.arange(number_of)

    def named(lengths, rotation):
        used = int((lengths > 0).sum())
        fixed = max(1, used // 4)
        shifted = fixed + (places - fixed + rotation * (used - fixed)) % max(1, number_of - fixed)
        return jnp.zeros((number_of,), jnp.int32).at[order[jnp.where(places < fixed, places, shifted)]].set(jnp.asarray(lengths, jnp.int32))

    lengths = jnp.where(number % 4 == 0, named(packed, number // 4), named(common, number - number // 4 - 1))
    mixed = jax.random.permutation(jax.random.fold_in(own, 3), number_of)
    donor, taker = mixed[0:number_of // 2 * 2:2], mixed[1:number_of // 2 * 2:2]
    room = jnp.minimum(lengths[donor] - 1, bound - lengths[taker]) // 2
    room = jnp.where((donor == order[0]) | (taker == order[0]) | (lengths[taker] == 0), 0, jnp.maximum(room, 0))
    shifted = jax.random.randint(jax.random.fold_in(own, 4), (number_of // 2,), 0, 1 << 20) % (room + 1)
    lengths = lengths.at[donor].add(-shifted).at[taker].add(shifted)
    members = jnp.searchsorted(jnp.cumsum(lengths), jnp.arange(rows * top), side="right").astype(jnp.int32)
    listing = members.reshape(top, rows).T
    listing = listing[jax.random.permutation(jax.random.fold_in(own, 1), rows)]
    rotation = jax.random.randint(jax.random.fold_in(own, 2), (rows, 1), 0, top)
    return jnp.take_along_axis(listing, (jnp.arange(top)[None, :] + rotation) % top, axis=1)


def portions_of(amount, total, bound, slope, full):
    weights = [(1 << 20) // math.isqrt(rank ** slope) + 1 for rank in range(1, amount + 1)]
    largest = bound if full else min(bound, max(-(-total // amount), total * weights[0] // sum(weights)))
    least = 1 if total - largest >= amount - 1 else 0
    holding, surplus = [largest] + [least] * (amount - 1), total - largest - least * (amount - 1)
    while surplus > 0:
        free = [i for i in range(1, amount) if holding[i] < largest] or [i for i in range(1, amount) if holding[i] < bound]
        whole, budget = sum([weights[i] for i in free]), surplus
        for i in free:
            extra = min(bound - holding[i], max(1, budget * weights[i] // whole), surplus)
            holding[i] = holding[i] + extra
            surplus = surplus - extra
    return np.array(holding)


def centred(own_key, shape, scale, limit, split=(), kind=jnp.bfloat16):
    drawn = jax.random.normal(own_key, shape, jnp.float32) * scale
    if len(split) > 0:
        drawn = block_scale(own_key, shape, split, -0.22, 0.18) * drawn
    return jnp.clip(drawn, min=-limit, max=limit).astype(kind)


def setup_inputs(seed: int = 0) -> dict:
    key_list = jax.random.split(jax.random.key(seed), 17)
    skip_stream_entering = centred(key_list[0], (BATCH_SAMPLES, TIME_STEPS, D), 1.0, 6.0, ((0, 4), (1, 8)))
    mapped_probe_matrix = centred(key_list[1], (BATCH_SAMPLES, TIME_STEPS, ATTENTION_GROUPS * KEY_WIDTH), 1.0, 6.0, ((0, 4), (1, 8)))
    mapped_lookup_matrix = centred(key_list[2], (BATCH_SAMPLES, TIME_STEPS, ATTENTION_GROUPS * KEY_WIDTH), 1.0, 6.0, ((0, 4), (1, 8)))
    mapped_content_matrix = centred(key_list[3], (BATCH_SAMPLES, TIME_STEPS, ATTENTION_GROUPS * DV), 1.0, 6.0, ((0, 4), (1, 8)))
    retention_preactivation = draw_retention_preactivation(jax.random.fold_in(key_list[16], 71), 0)
    extra_shrinkage = draw_extra_shrinkage(jax.random.fold_in(key_list[16], 71), 0)
    attention_group_scale = jnp.clip(1.0 + 0.18 * jax.random.normal(key_list[6], (ATTENTION_GROUPS * DV,), jnp.float32), 0.1, 1.9)
    final_projection_matrix = centred(key_list[7], (ATTENTION_GROUPS * DV, D), (ATTENTION_GROUPS * DV) ** -0.5, 0.09375, ((1, 4),))
    blender_branch_scale = jnp.clip(1.0 + 0.18 * jax.random.normal(key_list[8], (D,), jnp.float32), 0.1, 1.9)
    specialist_prenormal_scale = jnp.clip(1.0 + 0.18 * jax.random.normal(key_list[9], (D,), jnp.float32), 0.1, 1.9)
    specialist_switch_matrix = centred(key_list[10], (EXPERTS, D, FF), D ** -0.5, 0.125, ((0, 32),))
    specialist_expand_matrix = centred(key_list[11], (EXPERTS, D, FF), D ** -0.5, 0.125, ((0, 32),))
    specialist_contract_matrix = centred(key_list[12], (EXPERTS, FF, D), FF ** -0.5, 0.1875, ((0, 32),))
    specialist_branch_scale = jnp.clip(1.0 + 0.18 * jax.random.normal(key_list[13], (D,), jnp.float32), 0.1, 1.9)
    assigned_specialists_keys = jax.random.split(jax.random.fold_in(key_list[14], 1), BATCH_SAMPLES * TIME_STEPS // TOK_DEV)
    assigned_specialists_turns = jax.random.permutation(jax.random.fold_in(key_list[14], 3), BATCH_SAMPLES * TIME_STEPS // TOK_DEV)
    assigned_specialists = jax.vmap(lambda own, number: assign_block(jax.random.fold_in(key_list[14], 2), own, number, TOK_DEV, EXPERTS, TOP, CAP, 2))(assigned_specialists_keys, assigned_specialists_turns).reshape((BATCH_SAMPLES, TIME_STEPS, TOP))
    dispatcher_logits = jnp.clip(jnp.exp(math.log(1.0) - 1.609438 * jax.random.uniform(key_list[15], (BATCH_SAMPLES, TIME_STEPS, TOP), jnp.float32) ** block_scale(key_list[15], (BATCH_SAMPLES, TIME_STEPS, TOP), ((0, 4), (1, 8)), -0.2, 0.2)), 0.2, 1.0)
    return dict(skip_stream_entering=skip_stream_entering, mapped_probe_matrix=mapped_probe_matrix, mapped_lookup_matrix=mapped_lookup_matrix, mapped_content_matrix=mapped_content_matrix, retention_preactivation=retention_preactivation, extra_shrinkage=extra_shrinkage, attention_group_scale=attention_group_scale, final_projection_matrix=final_projection_matrix, blender_branch_scale=blender_branch_scale, specialist_prenormal_scale=specialist_prenormal_scale, specialist_switch_matrix=specialist_switch_matrix, specialist_expand_matrix=specialist_expand_matrix, specialist_contract_matrix=specialist_contract_matrix, specialist_branch_scale=specialist_branch_scale, assigned_specialists=assigned_specialists, dispatcher_logits=dispatcher_logits)


epsilon = 1e-06
softness_factor = 16.0
highest = lax.Precision.HIGHEST

def rms_scale(values, gain):
    mean_square = lax.optimization_barrier(jnp.mean(values * values, axis=-1, keepdims=True))
    return values * lax.rsqrt(mean_square + epsilon) * gain

def combine_states(earlier, later):
    return (earlier[0] * later[0], later[0][..., None] * earlier[1] + later[1])

def block_attention(query_f, key_f, value_f, shrink_exponent):
    length_value, head_count, key_dim = query_f.shape
    value_dim = value_f.shape[-1]
    block_count = length_value // BLOCK
    query_blocks = query_f.reshape(block_count, BLOCK, head_count, key_dim)
    key_blocks = key_f.reshape(block_count, BLOCK, head_count, key_dim)
    value_blocks = value_f.reshape(block_count, BLOCK, head_count, value_dim)
    within = jnp.cumsum(shrink_exponent.reshape(block_count, BLOCK, head_count, key_dim), axis=1)
    block_end = within[:, -1]
    lifted = query_blocks * jnp.exp(within)
    lowered = key_blocks * jnp.exp(-within)
    scores = jnp.einsum('nthk,nshk->nhts', lifted, lowered, precision=highest)
    causal = jnp.arange(BLOCK)[:, None] >= jnp.arange(BLOCK)[None, :]
    scores = jnp.where(causal, scores, 0.0)
    inside = jnp.einsum('nhts,nshv->nthv', scores, value_blocks, precision=highest)
    carried_keys = key_blocks * jnp.exp(block_end[:, None] - within)
    updates = jnp.einsum('nshk,nshv->nhkv', carried_keys, value_blocks, precision=highest)
    decays = jnp.exp(block_end)
    total_decay, states = lax.associative_scan(combine_states, (decays, updates), axis=0)
    entering = jnp.concatenate([jnp.zeros_like(states[:1]), states[:-1]], axis=0)
    across = jnp.einsum('nthk,nhkv->nthv', lifted, entering, precision=highest)
    outputs = (inside + across).reshape(length_value, head_count, value_dim)
    offsets = jnp.cumsum(block_end, axis=0) - block_end
    reached = (query_blocks * jnp.exp(within + offsets[:, None])).reshape(length_value, head_count, key_dim)
    return (outputs, total_decay[-1], states[-1], reached)

def reference(skip_stream_entering, mapped_probe_matrix, mapped_lookup_matrix, mapped_content_matrix, retention_preactivation, extra_shrinkage, attention_group_scale, final_projection_matrix, blender_branch_scale, specialist_prenormal_scale, specialist_switch_matrix, specialist_expand_matrix, specialist_contract_matrix, specialist_branch_scale, assigned_specialists, dispatcher_logits):

    def lone_series(fragment_array):
        probe_series, lookup_series, content_series, shrink_series, spike_series = fragment_array
        length_value = probe_series.shape[0]
        query_f = probe_series.reshape(length_value, ATTENTION_GROUPS, KEY_WIDTH).astype(jnp.float32) * KEY_WIDTH ** (-0.5)
        key_f = lookup_series.reshape(length_value, ATTENTION_GROUPS, KEY_WIDTH).astype(jnp.float32)
        value_f = content_series.reshape(length_value, ATTENTION_GROUPS, DV).astype(jnp.float32)
        shrink_exponent = jax.nn.log_sigmoid(shrink_series.reshape(length_value, ATTENTION_GROUPS, KEY_WIDTH).astype(jnp.float32)) / softness_factor
        shrink_exponent = shrink_exponent + jnp.transpose(spike_series)[:, :, None]
        outputs = block_attention(query_f, key_f, value_f, shrink_exponent)[0]
        return rms_scale(outputs, attention_group_scale.reshape(ATTENTION_GROUPS, DV)).astype(jnp.bfloat16)
    attention_group_result = lax.map(lone_series, (mapped_probe_matrix, mapped_lookup_matrix, mapped_content_matrix, retention_preactivation, extra_shrinkage))
    token_count = BATCH_SAMPLES * TIME_STEPS
    attention_group_result = attention_group_result.reshape(token_count, ATTENTION_GROUPS * DV)
    projected = jnp.dot(attention_group_result, final_projection_matrix, preferred_element_type=jnp.float32).astype(jnp.bfloat16)
    stream = skip_stream_entering.reshape(token_count, D).astype(jnp.float32)
    residual = (stream + rms_scale(projected.astype(jnp.float32), blender_branch_scale)).astype(jnp.bfloat16)
    expert_in = rms_scale(residual.astype(jnp.float32), specialist_prenormal_scale).astype(jnp.bfloat16)
    block_total = token_count // TOK_DEV
    pair_dev = TOK_DEV * TOP
    pair_count = token_count * TOP
    chosen = assigned_specialists.reshape(block_total, pair_dev)
    onehot = (chosen[:, :, None] == jnp.arange(EXPERTS, dtype=jnp.int32)[None, None, :]).astype(jnp.int32)
    ranks = lax.optimization_barrier(jnp.sum((jnp.cumsum(onehot, axis=1) - onehot) * onehot, axis=2))
    block_ids = jnp.arange(block_total, dtype=jnp.int32)[:, None]
    slots = (chosen * block_total + block_ids) * CAP + ranks
    pair_ids = jnp.arange(pair_count, dtype=jnp.int32)
    table = jnp.full((EXPERTS * block_total * CAP,), pair_count, jnp.int32)
    table = table.at[slots.reshape(-1)].set(pair_ids).reshape(EXPERTS, block_total * CAP)
    padded = jnp.concatenate([expert_in, jnp.zeros((1, D), jnp.bfloat16)], axis=0)

    def expert_step(carry, fragment_array):
        sources, gate_weight, up_weight, down_weight = fragment_array
        row_block = padded[sources // TOP]
        gate_part = jnp.dot(row_block, gate_weight, preferred_element_type=jnp.float32)
        up_part = jnp.dot(row_block, up_weight, preferred_element_type=jnp.float32)
        hidden_units = (jax.nn.silu(gate_part) * up_part).astype(jnp.bfloat16)
        result = jnp.dot(hidden_units, down_weight, preferred_element_type=jnp.float32).astype(jnp.bfloat16)
        return (carry.at[sources].set(result, mode='drop'), None)
    pair_out, _ = lax.scan(expert_step, jnp.zeros((pair_count, D), jnp.bfloat16), (table, specialist_switch_matrix, specialist_expand_matrix, specialist_contract_matrix))
    weights = dispatcher_logits.reshape(token_count, TOP)
    weights = weights / lax.optimization_barrier(jnp.sum(weights, axis=1, keepdims=True))
    combined = lax.optimization_barrier(jnp.sum(pair_out.reshape(token_count, TOP, D).astype(jnp.float32) * weights[:, :, None], axis=1))
    layer_out = residual.astype(jnp.float32) + rms_scale(combined, specialist_branch_scale)
    return layer_out.astype(jnp.bfloat16).reshape(BATCH_SAMPLES, TIME_STEPS, D)
```

```python
import functools

import jax
import jax.numpy as jnp
from jax import lax
from jax.experimental import pallas as pl
from jax.experimental.pallas import tpu as pltpu
from jax.sharding import PartitionSpec as P

D = 2048
KEY_WIDTH = 128
DV = 256
TOP = 2
BLOCK = 64


epsilon = 1e-06
softness_factor = 16.0


def rms_scale(values, gain):
    mean_square = jnp.mean(values * values, axis=-1, keepdims=True)
    return values * lax.rsqrt(mean_square + epsilon) * gain


PLANES = 4
LANES = 128
MESH = pl.DeviceIdType.MESH


def pair_rows(h, width):
    return pl.ds(pl.multiple_of(h * width, width), width)


def layer_kernel(
    q_hbm, k_hbm, v_hbm, g_hbm, stream_hbm, w_hbm, gate_hbm, up_hbm, down_hbm,
    extra_ref, gain_ref, branch_ref, pre_ref, post_ref, chosen_ref, logits_ref, out_ref,
    q_ref, k_ref, v_ref, g_ref, stream_ref, w_buf, extras, within, lifted, lowered, reached, inside,
    states_out, states, decays_out, decays, entering, onward, crossed, own_heads, peer_heads,
    proj_out, proj,
    load_sem, w_sem, extra_send, extra_recv, state_send, state_recv, decay_send, decay_recv,
    chain_send, chain_recv, cross_send, cross_recv, head_send, head_recv, proj_send, proj_recv,
    residuals, tokens, outgoing, arrivals, results, returned, combined, gate_w, up_w, down_w,
    route_rows, source_rows, slots, sources, shares,
    weight_sem, route_sem, row_send, row_recv, back_send, back_recv,
):
    sp_count, dp_count = lax.axis_size("sp"), lax.axis_size("dp")
    sp, dp = lax.axis_index("sp"), lax.axis_index("dp")
    pair, side = sp // 2, lax.rem(sp, 2)
    pairs = sp_count // 2
    y, core = dp // 2, lax.rem(dp, 2)
    ys = dp_count // 2
    rows = q_ref.shape[0]
    heads = q_ref.shape[1] // KEY_WIDTH
    half = heads // 2
    own = extra_ref.shape[0]
    cols = w_hbm.shape[1]
    partner = (sp + 1 - 2 * side, dp)
    twin = (sp, dp + 1 - 2 * core)

    def remote(src, dst, send, recv, where):
        return pltpu.make_async_remote_copy(
            src_ref=src, dst_ref=dst, send_sem=send, recv_sem=recv,
            device_id=where, device_id_type=MESH,
        )

    def peer_y(k):
        return (sp, lax.rem(y + k, ys) * 2 + core)

    loads = [
        pltpu.make_async_copy(src, dst, load_sem.at[i])
        for i, (src, dst) in enumerate(
            ((g_hbm, g_ref), (k_hbm, k_ref), (v_hbm, v_ref), (q_hbm, q_ref),
             (stream_hbm, stream_ref), (w_hbm, w_buf.at[core]))
        )
    ]
    for copy in loads:
        copy.start()

    total = sp_count * dp_count
    me = sp * dp_count + dp
    cap = outgoing.shape[1]
    per = total // PLANES
    plane, place = me // per, lax.rem(me, per)

    def where_is(peer):
        return (peer // dp_count, lax.rem(peer, dp_count))

    barrier = pltpu.get_barrier_semaphore()

    @pl.loop(1, total)
    def _(i):
        peer = lax.rem(me + i, total)
        pl.semaphore_signal(barrier, inc=1, device_id=where_is(peer), device_id_type=MESH)

    row = lax.broadcasted_iota(jnp.int32, (rows, rows), 0)
    col = lax.broadcasted_iota(jnp.int32, (rows, rows), 1)
    causal = row >= col
    ones = jnp.where(causal, 1.0, 0.0).astype(jnp.bfloat16)
    ones = jnp.concatenate([ones, ones], axis=1)

    expert = lax.broadcasted_iota(jnp.int32, (total, rows), 0)
    picks = [chosen_ref[j : j + 1] for j in range(TOP)]
    named = functools.reduce(jnp.logical_or, [expert == pick for pick in picks])
    before = jnp.dot(
        jnp.where(named, 1.0, 0.0).astype(jnp.bfloat16),
        jnp.where(row < col, 1.0, 0.0).astype(jnp.bfloat16),
        preferred_element_type=jnp.float32,
    )
    spot = lax.broadcasted_iota(jnp.int32, (rows, source_rows.shape[1]), 1).astype(jnp.float32)
    token = lax.broadcasted_iota(jnp.int32, spot.shape, 0).astype(jnp.float32)
    source = jnp.zeros(spot.shape, jnp.float32)
    for j, pick in enumerate(picks):
        rank = jnp.sum(jnp.where(expert == pick, before, 0.0), axis=0, keepdims=True)
        slot = pick.astype(jnp.float32) * cap + rank
        route_rows[j : j + 1] = pick
        route_rows[TOP + j : TOP + j + 1] = jnp.clip(rank.astype(jnp.int32), 0, cap - 1)
        upright = jnp.sum(jnp.where(row == col, slot, 0.0), axis=1, keepdims=True)
        source = source + jnp.where(spot == upright, token, 0.0)
    source = jnp.sum(source, axis=0, keepdims=True).astype(jnp.int32)
    source_rows[...] = jnp.clip(source, 0, rows - 1)
    loads[0].wait()

    @pl.loop(0, half)
    def _(j):
        cut = pair_rows(j, 2 * KEY_WIDTH)
        g = g_ref[:, cut].astype(jnp.float32)
        logs = (jnp.minimum(g, 0.0) - jnp.log(1.0 + jnp.exp(-jnp.abs(g)))) / softness_factor
        high = logs.astype(jnp.bfloat16)
        low = (logs - high.astype(jnp.float32)).astype(jnp.bfloat16)
        within[:, cut] = jnp.dot(
            ones, jnp.concatenate([high, low], axis=0), preferred_element_type=jnp.float32
        )

    tables = [
        pltpu.make_async_copy(src, dst, route_sem.at[i])
        for i, (src, dst) in enumerate(
            ((route_rows, slots), (source_rows, sources), (logits_ref, shares))
        )
    ]
    for copy in tables:
        copy.start()
    pl.semaphore_wait(barrier, total - 1)

    @pl.loop(1, sp_count)
    def _(i):
        peer = lax.rem(sp + i, sp_count)
        remote(
            extra_ref.at[:, pair_rows(peer, rows)], extras.at[sp], extra_send, extra_recv, (peer, dp)
        ).start()

    pltpu.make_async_copy(
        extra_ref.at[:, pair_rows(sp, rows)], extras.at[sp], extra_recv
    ).start()
    w_copy = remote(w_hbm, w_buf.at[core], w_sem.at[0], w_sem.at[1], twin)
    w_copy.start()

    @pl.when(pair == 0)
    def _():
        entering[0] = jnp.zeros(entering.shape[1:], entering.dtype)

    for copy in loads[1:4]:
        copy.wait()
    weights = [
        pltpu.make_async_copy(src.at[0], dst, weight_sem.at[i])
        for i, (src, dst) in enumerate(
            ((gate_hbm, gate_w), (up_hbm, up_w), (down_hbm, down_w))
        )
    ]
    for copy in weights:
        copy.start()
    pltpu.make_async_copy(extras, extras, extra_recv).wait()

    def local_state(h):
        cut = pair_rows(h, KEY_WIDTH)
        extra = jnp.sum(
            jnp.where(causal, extras[h // own, pl.ds(lax.rem(h, own), 1)], 0.0),
            axis=1, keepdims=True,
        )
        b = within[:, cut] + extra
        middle = b[rows // 2 - 1 : rows // 2]
        end = b[rows - 1 : rows]
        up = jnp.exp(b - middle)
        down = jnp.exp(middle - b)
        q = q_ref[:, cut].astype(jnp.float32) * (KEY_WIDTH ** (-0.5)) * up
        k = k_ref[:, cut].astype(jnp.float32) * down
        lifted[:, cut] = q.astype(jnp.bfloat16)
        lowered[:, cut] = k.astype(jnp.bfloat16)
        reached[:, cut] = (q * jnp.exp(middle)).astype(jnp.bfloat16)
        carried = (k * jnp.exp(end - middle)).astype(jnp.bfloat16)
        state = lax.dot_general(
            v_ref[:, pair_rows(h, DV)], carried, (((0,), (0,)), ((), ())),
            preferred_element_type=jnp.float32,
        )
        return state.astype(jnp.bfloat16), jnp.exp(end)

    @pl.loop(0, half // 2)
    def _(j):
        for i in (2 * j, 2 * j + 1):
            state, decay = local_state((1 - side) * half + i)
            states_out[i] = state
            decays_out[i] = decay
        for i in (2 * j, 2 * j + 1):
            remote(
                states_out.at[i], states.at[side, i], state_send, state_recv.at[i], partner
            ).start()

    decay_copy = remote(decays_out, decays.at[side], decay_send, decay_recv, partner)
    decay_copy.start()

    @pl.loop(0, half // 2)
    def _(j):
        for i in (2 * j, 2 * j + 1):
            state, decay = local_state(side * half + i)
            states[side, i] = state
            decays[side, i] = decay

    @pl.loop(0, half)
    def _(j):
        for h in (2 * j, 2 * j + 1):
            cut = pair_rows(h, KEY_WIDTH)
            wide = pair_rows(h, DV)
            scores = lax.dot_general(
                lifted[:, cut], lowered[:, cut], (((1,), (1,)), ((), ())),
                preferred_element_type=jnp.float32,
            )
            scores = jnp.where(causal, scores, 0.0).astype(jnp.bfloat16)
            inside[:, wide] = jnp.dot(scores, v_ref[:, wide], preferred_element_type=jnp.float32)

    def finish(h, state):
        wide = pair_rows(h, DV)
        mixed = inside[:, wide] + lax.dot_general(
            reached[:, pair_rows(h, KEY_WIDTH)], state, (((1,), (1,)), ((), ())),
            preferred_element_type=jnp.float32,
        )
        own_heads[h] = rms_scale(mixed, gain_ref[:, wide]).astype(jnp.bfloat16)
        for k in range(1, ys):
            remote(
                own_heads.at[h], peer_heads.at[k - 1, h],
                head_send.at[k - 1], head_recv.at[k - 1, h], peer_y(k),
            ).start()

    def finish_crossed(i):
        pltpu.make_async_copy(crossed.at[i], crossed.at[i], cross_recv.at[i]).wait()
        finish((1 - side) * half + i, crossed[i])

    lag = 2
    remote(decays_out, decays.at[side], decay_send, decay_recv, partner).wait_recv()

    @pl.loop(0, half)
    def _(i):
        pltpu.make_async_copy(
            states_out.at[i], states_out.at[i], state_recv.at[i]
        ).wait()

        @pl.when(pair > 0)
        def _():
            pltpu.make_async_copy(onward.at[i], onward.at[i], chain_recv.at[i]).wait()

        middle = entering[0, i].astype(jnp.float32) * decays[0, i] + states[0, i].astype(jnp.float32)
        entering[1, i] = middle.astype(jnp.bfloat16)
        onward[i] = (middle * decays[1, i] + states[1, i].astype(jnp.float32)).astype(jnp.bfloat16)

        @pl.when(pair < pairs - 1)
        def _():
            remote(
                onward.at[i], entering.at[0, i], chain_send, chain_recv.at[i], (sp + 2, dp)
            ).start()

        remote(
            entering.at[1 - side, i], crossed.at[i], cross_send, cross_recv.at[i], partner
        ).start()
        finish(side * half + i, entering[side, i])

        @pl.when(i >= lag)
        def _():
            finish_crossed(i - lag)

    @pl.loop(half - lag, half)
    def _(i):
        finish_crossed(i)

    loads[5].wait()
    w_copy.wait_recv()

    def project(head_of, ready):
        total = None
        for h in range(heads):
            ready(h)
            wide = pl.ds(h * DV, DV)
            part = [
                jnp.dot(head_of(h), w_buf[c, wide, :], preferred_element_type=jnp.float32)
                for c in range(2)
            ]
            total = part if total is None else [a + b for a, b in zip(total, part)]
        return jnp.concatenate(total, axis=1).astype(jnp.bfloat16)

    for k in range(1, ys):
        def ready(h, k=k):
            pltpu.make_async_copy(
                peer_heads.at[k - 1, h], peer_heads.at[k - 1, h], head_recv.at[k - 1, h]
            ).wait()

        proj_out[k - 1] = project(lambda h, k=k: peer_heads[k - 1, h], ready)
        back = (sp, lax.rem(y - k + ys, ys) * 2 + core)
        remote(proj_out.at[k - 1], proj.at[y], proj_send, proj_recv, back).start()
    proj[y] = project(lambda h: own_heads[h], lambda h: None)
    loads[4].wait()
    arrived = proj.at[pl.ds(0, ys - 1)]
    pltpu.make_async_copy(arrived, arrived, proj_recv).wait()
    projected = jnp.concatenate([proj[i] for i in range(ys)], axis=1).astype(jnp.float32)
    residual = stream_ref[...].astype(jnp.float32) + rms_scale(projected, branch_ref[...])
    residual = residual.astype(jnp.bfloat16)
    residuals[...] = residual
    inputs = rms_scale(residual.astype(jnp.float32), pre_ref[...]).astype(jnp.bfloat16)
    segments = D // LANES
    tokens[...] = inputs.reshape(rows, segments, LANES)
    for copy in tables:
        copy.wait()

    def group_of(step):
        across = lax.rem(plane + step // 2 * 2, PLANES)
        return across + lax.rem(step, 2) * (1 - 2 * lax.rem(across, 2))

    def block(ref, peer):
        return ref.at[peer]

    @pl.loop(0, total)
    def _(i):
        group = group_of(lax.rem(i // per + 2, PLANES))
        peer = group * per + lax.rem(place + lax.rem(i, per), per)
        for r in range(cap):
            outgoing[peer, r] = tokens[jnp.clip(sources[0, peer * cap + r], 0, rows - 1)]

        @pl.when(peer != me)
        def _():
            remote(
                block(outgoing, peer), block(arrivals, me), row_send, row_recv.at[plane],
                where_is(peer),
            ).start()

        @pl.when(peer == me)
        def _():
            pltpu.make_async_copy(
                block(outgoing, me), block(arrivals, me), row_recv.at[plane]
            ).start()

    for copy in weights:
        copy.wait()

    @pl.loop(0, PLANES)
    def _(step):
        group = group_of(step)
        base = group * per
        batch = pl.ds(base, per)
        pltpu.make_async_copy(arrivals.at[batch], arrivals.at[batch], row_recv.at[group]).wait()
        x = arrivals[batch].reshape(per * cap, D)
        gate_part = jnp.dot(x, gate_w[...], preferred_element_type=jnp.float32)
        up_part = jnp.dot(x, up_w[...], preferred_element_type=jnp.float32)
        hidden = (jax.nn.silu(gate_part) * up_part).astype(jnp.bfloat16)
        result = jnp.dot(hidden, down_w[...], preferred_element_type=jnp.float32)
        results[batch] = result.astype(jnp.bfloat16).reshape(per, cap, segments, LANES)

        @pl.loop(0, per)
        def _(j):
            peer = base + lax.rem(place + j, per)

            @pl.when(peer != me)
            def _():
                remote(
                    block(results, peer), block(returned, me), back_send, back_recv,
                    where_is(peer),
                ).start()

            @pl.when(peer == me)
            def _():
                pltpu.make_async_copy(
                    block(results, me), block(returned, me), back_recv
                ).start()

    pltpu.make_async_copy(returned, returned, back_recv).wait()

    @pl.loop(0, rows // 8)
    def _(i):
        for t in range(8):
            at = i * 8 + t
            first, second = shares[0, at], shares[1, at]
            both = first + second
            rows_of = [
                returned[
                    jnp.clip(slots[j, at], 0, total - 1), jnp.clip(slots[TOP + j, at], 0, cap - 1)
                ].astype(jnp.float32)
                for j in range(TOP)
            ]
            combined[at] = rows_of[0] * (first / both) + rows_of[1] * (second / both)

    routed = rms_scale(combined[...].reshape(rows, D), post_ref[...])
    out_ref[...] = (residuals[...].astype(jnp.float32) + routed).astype(jnp.bfloat16)

    others = pl.ds(0, total - 1)
    pltpu.make_async_copy(outgoing.at[others], outgoing.at[others], row_send).wait()
    pltpu.make_async_copy(results.at[others], results.at[others], back_send).wait()

    sent = extras.at[pl.ds(0, sp_count - 1)]
    pltpu.make_async_copy(sent, sent, extra_send).wait()
    pltpu.make_async_copy(states_out, states_out, state_send).wait()
    decay_copy.wait_send()
    w_copy.wait_send()
    pltpu.make_async_copy(crossed, crossed, cross_send).wait()

    @pl.when(pair < pairs - 1)
    def _():
        pltpu.make_async_copy(onward, onward, chain_send).wait()

    for k in range(1, ys):
        pltpu.make_async_copy(own_heads, own_heads, head_send.at[k - 1]).wait()
    pltpu.make_async_copy(proj_out, proj_out, proj_send).wait()


def layer(
    query, key, value, gate, stream, weight, gate_weight, up_weight, down_weight,
    extra, gain, branch_gain, pre_gain, post_gain, chosen, logits,
):
    rows, width = query.shape
    heads = width // KEY_WIDTH
    half = heads // 2
    sp_count, dp_count = lax.axis_size("sp"), lax.axis_size("dp")
    ys = dp_count // 2
    total = sp_count * dp_count
    cols = weight.shape[1]
    cap = max(2, 5 * rows * TOP // (3 * total))
    bf16, f32, i32 = jnp.bfloat16, jnp.float32, jnp.int32
    vmem = pl.BlockSpec(memory_space=pltpu.VMEM)
    anywhere = pl.BlockSpec(memory_space=pl.ANY)
    state = (DV, KEY_WIDTH)
    table = (1, -(-total * cap // LANES) * LANES)
    units = pltpu.VMEM((total, cap, D // LANES, LANES), bf16)
    dma = pltpu.SemaphoreType.DMA
    return pl.pallas_call(
        layer_kernel,
        in_specs=[anywhere] * 9 + [vmem] * 7,
        out_specs=vmem,
        out_shape=jax.ShapeDtypeStruct((rows, D), bf16),
        scratch_shapes=[
            pltpu.VMEM((rows, width), bf16),
            pltpu.VMEM((rows, width), bf16),
            pltpu.VMEM(value.shape, bf16),
            pltpu.VMEM((rows, width), bf16),
            pltpu.VMEM((rows, D), bf16),
            pltpu.VMEM((2,) + weight.shape, bf16),
            pltpu.VMEM((sp_count, extra.shape[0], rows), f32),
            pltpu.VMEM((rows, width), f32),
            pltpu.VMEM((rows, width), bf16),
            pltpu.VMEM((rows, width), bf16),
            pltpu.VMEM((rows, width), bf16),
            pltpu.VMEM(value.shape, f32),
            pltpu.VMEM((half,) + state, bf16),
            pltpu.VMEM((2, half) + state, bf16),
            pltpu.VMEM((half, 1, KEY_WIDTH), f32),
            pltpu.VMEM((2, half, 1, KEY_WIDTH), f32),
            pltpu.VMEM((2, half) + state, bf16),
            pltpu.VMEM((half,) + state, bf16),
            pltpu.VMEM((half,) + state, bf16),
            pltpu.VMEM((heads, rows, DV), bf16),
            pltpu.VMEM((ys - 1, heads, rows, DV), bf16),
            pltpu.VMEM((ys - 1, rows, 2 * cols), bf16),
            pltpu.VMEM((ys, rows, 2 * cols), bf16),
            dma((6,)), dma((2,)), dma, dma, dma, dma((half,)), dma, dma,
            dma, dma((half,)), dma, dma((half,)), dma((ys - 1,)), dma((ys - 1, heads)), dma, dma,
            pltpu.VMEM((rows, D), bf16),
            pltpu.VMEM((rows, D // LANES, LANES), bf16),
            units, units, units, units,
            pltpu.VMEM((rows, D // LANES, LANES), f32),
            *[pltpu.VMEM(w.shape[1:], bf16) for w in (gate_weight, up_weight, down_weight)],
            pltpu.VMEM((2 * TOP, rows), i32),
            pltpu.VMEM(table, i32),
            pltpu.SMEM((2 * TOP, rows), i32),
            pltpu.SMEM(table, i32),
            pltpu.SMEM((TOP, rows), f32),
            dma((3,)), dma((3,)), dma, dma((PLANES,)), dma, dma,
        ],
        compiler_params=pltpu.CompilerParams(
            collective_id=0, has_side_effects=True, vmem_limit_bytes=60 * 1024 * 1024
        ),
        name="layer",
    )(
        query, key, value, gate, stream, weight, gate_weight, up_weight, down_weight,
        extra, gain.reshape(1, -1), branch_gain.reshape(1, -1), pre_gain.reshape(1, -1),
        post_gain.reshape(1, -1), chosen, logits,
    )


def shards(
    skip_stream_entering,
    mapped_probe_matrix,
    mapped_lookup_matrix,
    mapped_content_matrix,
    retention_preactivation,
    extra_shrinkage,
    attention_group_scale,
    final_projection_matrix,
    blender_branch_scale,
    specialist_prenormal_scale,
    specialist_switch_matrix,
    specialist_expand_matrix,
    specialist_contract_matrix,
    specialist_branch_scale,
    assigned_specialists,
    dispatcher_logits,
):
    out = layer(
        mapped_probe_matrix[0],
        mapped_lookup_matrix[0],
        mapped_content_matrix[0],
        retention_preactivation[0],
        skip_stream_entering[0],
        final_projection_matrix,
        specialist_switch_matrix,
        specialist_expand_matrix,
        specialist_contract_matrix,
        extra_shrinkage[0],
        attention_group_scale,
        blender_branch_scale,
        specialist_prenormal_scale,
        specialist_branch_scale,
        jnp.transpose(assigned_specialists[0]),
        jnp.transpose(dispatcher_logits[0]),
    )
    return out[None]


def solution(mesh):
    return jax.shard_map(
        shards,
        mesh=mesh,
        in_specs=(
            P("dp", "sp", None),
            P("dp", "sp", None),
            P("dp", "sp", None),
            P("dp", "sp", None),
            P("dp", "sp", None),
            P("dp", "sp", None),
            P(),
            P(None, "dp"),
            P(),
            P(),
            P(("sp", "dp"), None, None),
            P(("sp", "dp"), None, None),
            P(("sp", "dp"), None, None),
            P(),
            P("dp", "sp", None),
            P("dp", "sp", None),
        ),
        out_specs=P("dp", "sp", None),
        check_vma=False,
    )
```

```python
import functools

import jax
import jax.numpy as jnp
from jax import lax
from jax.experimental import pallas as pl
from jax.experimental.pallas import tpu as pltpu
from jax.sharding import PartitionSpec as P

D = 2048
KEY_WIDTH = 128
DV = 256
TOP = 2
BLOCK = 64


epsilon = 1e-06
softness_factor = 16.0


def rms_scale(values, gain):
    mean_square = jnp.mean(values * values, axis=-1, keepdims=True)
    return values * lax.rsqrt(mean_square + epsilon) * gain


PLANES = 4
LANES = 128
MESH = pl.DeviceIdType.MESH


def pair_rows(h, width):
    return pl.ds(pl.multiple_of(h * width, width), width)


def layer_kernel(
    q_hbm, k_hbm, v_hbm, g_hbm, stream_hbm, w_hbm, gate_hbm, up_hbm, down_hbm,
    extra_ref, gain_ref, branch_ref, pre_ref, post_ref, chosen_ref, logits_ref, out_ref,
    q_ref, k_ref, v_ref, g_ref, stream_ref, w_buf, extras, within, lifted, lowered, reached, inside,
    states_out, states, decays_out, decays, entering, onward, crossed, own_heads, peer_heads,
    proj_out, proj,
    load_sem, w_sem, extra_send, extra_recv, state_send, state_recv, decay_send, decay_recv,
    chain_send, chain_recv, cross_send, cross_recv, head_send, head_recv, proj_send, proj_recv,
    residuals, tokens, outgoing, arrivals, results, returned, combined, gate_w, up_w, down_w,
    route_rows, source_rows, share_rows, slots, sources, shares,
    weight_sem, route_sem, row_send, row_recv, back_send, back_recv,
):
    sp_count, dp_count = lax.axis_size("sp"), lax.axis_size("dp")
    sp, dp = lax.axis_index("sp"), lax.axis_index("dp")
    pair, side = sp // 2, lax.rem(sp, 2)
    pairs = sp_count // 2
    y, core = dp // 2, lax.rem(dp, 2)
    ys = dp_count // 2
    rows = q_ref.shape[0]
    heads = q_ref.shape[1] // KEY_WIDTH
    half = heads // 2
    own = extra_ref.shape[0]
    cols = w_hbm.shape[1]
    partner = (sp + 1 - 2 * side, dp)
    twin = (sp, dp + 1 - 2 * core)

    def remote(src, dst, send, recv, where):
        return pltpu.make_async_remote_copy(
            src_ref=src, dst_ref=dst, send_sem=send, recv_sem=recv,
            device_id=where, device_id_type=MESH,
        )

    def peer_y(k):
        return (sp, lax.rem(y + k, ys) * 2 + core)

    loads = [
        pltpu.make_async_copy(src, dst, load_sem.at[i])
        for i, (src, dst) in enumerate(
            ((g_hbm, g_ref), (k_hbm, k_ref), (v_hbm, v_ref), (q_hbm, q_ref),
             (stream_hbm, stream_ref), (w_hbm, w_buf.at[core]))
        )
    ]
    for copy in loads:
        copy.start()

    total = sp_count * dp_count
    me = sp * dp_count + dp
    cap = outgoing.shape[1]
    per = total // PLANES
    plane, place = me // per, lax.rem(me, per)

    def where_is(peer):
        return (peer // dp_count, lax.rem(peer, dp_count))

    barrier = pltpu.get_barrier_semaphore()

    @pl.loop(1, total)
    def _(i):
        peer = lax.rem(me + i, total)
        pl.semaphore_signal(barrier, inc=1, device_id=where_is(peer), device_id_type=MESH)

    row = lax.broadcasted_iota(jnp.int32, (rows, rows), 0)
    col = lax.broadcasted_iota(jnp.int32, (rows, rows), 1)
    causal = row >= col
    ones = jnp.where(causal, 1.0, 0.0).astype(jnp.bfloat16)
    ones = jnp.concatenate([ones, ones], axis=1)

    expert = lax.broadcasted_iota(jnp.int32, (total, rows), 0)
    picks = [chosen_ref[j : j + 1] for j in range(TOP)]
    named = functools.reduce(jnp.logical_or, [expert == pick for pick in picks])
    before = jnp.dot(
        jnp.where(named, 1.0, 0.0).astype(jnp.bfloat16),
        jnp.where(row < col, 1.0, 0.0).astype(jnp.bfloat16),
        preferred_element_type=jnp.float32,
    )
    spot = lax.broadcasted_iota(jnp.int32, (rows, source_rows.shape[1]), 1).astype(jnp.float32)
    token = lax.broadcasted_iota(jnp.int32, spot.shape, 0).astype(jnp.float32)
    source = jnp.zeros(spot.shape, jnp.float32)
    for j, pick in enumerate(picks):
        rank = jnp.sum(jnp.where(expert == pick, before, 0.0), axis=0, keepdims=True)
        slot = pick.astype(jnp.float32) * cap + rank
        route_rows[j : j + 1] = pick
        route_rows[TOP + j : TOP + j + 1] = jnp.clip(rank.astype(jnp.int32), 0, cap - 1)
        upright = jnp.sum(jnp.where(row == col, slot, 0.0), axis=1, keepdims=True)
        source = source + jnp.where(spot == upright, token, 0.0)
    source = jnp.sum(source, axis=0, keepdims=True).astype(jnp.int32)
    source_rows[...] = jnp.clip(source, 0, rows - 1)
    loads[0].wait()

    @pl.loop(0, half)
    def _(j):
        cut = pair_rows(j, 2 * KEY_WIDTH)
        g = g_ref[:, cut].astype(jnp.float32)
        logs = (jnp.minimum(g, 0.0) - jnp.log(1.0 + jnp.exp(-jnp.abs(g)))) / softness_factor
        high = logs.astype(jnp.bfloat16)
        low = (logs - high.astype(jnp.float32)).astype(jnp.bfloat16)
        within[:, cut] = jnp.dot(
            ones, jnp.concatenate([high, low], axis=0), preferred_element_type=jnp.float32
        )

    logits = [logits_ref[j : j + 1] for j in range(TOP)]
    for j in range(TOP):
        share_rows[j : j + 1] = logits[j] / sum(logits)
    tables = [
        pltpu.make_async_copy(src, dst, route_sem.at[i])
        for i, (src, dst) in enumerate(
            ((route_rows, slots), (source_rows, sources), (share_rows, shares))
        )
    ]
    for copy in tables:
        copy.start()
    pl.semaphore_wait(barrier, total - 1)

    @pl.loop(1, sp_count)
    def _(i):
        peer = lax.rem(sp + i, sp_count)
        remote(
            extra_ref.at[:, pair_rows(peer, rows)], extras.at[sp], extra_send, extra_recv, (peer, dp)
        ).start()

    pltpu.make_async_copy(
        extra_ref.at[:, pair_rows(sp, rows)], extras.at[sp], extra_recv
    ).start()
    w_copy = remote(w_hbm, w_buf.at[core], w_sem.at[0], w_sem.at[1], twin)
    w_copy.start()

    @pl.when(pair == 0)
    def _():
        entering[0] = jnp.zeros(entering.shape[1:], entering.dtype)

    for copy in loads[1:4]:
        copy.wait()
    weights = [
        pltpu.make_async_copy(src.at[0], dst, weight_sem.at[i])
        for i, (src, dst) in enumerate(
            ((gate_hbm, gate_w), (up_hbm, up_w), (down_hbm, down_w))
        )
    ]
    for copy in weights:
        copy.start()
    pltpu.make_async_copy(extras, extras, extra_recv).wait()

    def local_state(h):
        cut = pair_rows(h, KEY_WIDTH)
        extra = jnp.sum(
            jnp.where(causal, extras[h // own, pl.ds(lax.rem(h, own), 1)], 0.0),
            axis=1, keepdims=True,
        )
        b = within[:, cut] + extra
        middle = b[rows // 2 - 1 : rows // 2]
        end = b[rows - 1 : rows]
        up = jnp.exp(b - middle)
        down = jnp.exp(middle - b)
        q = q_ref[:, cut].astype(jnp.float32) * (KEY_WIDTH ** (-0.5)) * up
        k = k_ref[:, cut].astype(jnp.float32) * down
        lifted[:, cut] = q.astype(jnp.bfloat16)
        lowered[:, cut] = k.astype(jnp.bfloat16)
        reached[:, cut] = (q * jnp.exp(middle)).astype(jnp.bfloat16)
        carried = (k * jnp.exp(end - middle)).astype(jnp.bfloat16)
        state = lax.dot_general(
            v_ref[:, pair_rows(h, DV)], carried, (((0,), (0,)), ((), ())),
            preferred_element_type=jnp.float32,
        )
        return state.astype(jnp.bfloat16), jnp.exp(end)

    @pl.loop(0, half // 2)
    def _(j):
        for i in (2 * j, 2 * j + 1):
            state, decay = local_state((1 - side) * half + i)
            states_out[i] = state
            decays_out[i] = decay
        for i in (2 * j, 2 * j + 1):
            remote(
                decays_out.at[i], decays.at[side, i], decay_send, decay_recv.at[i], partner
            ).start()
            remote(
                states_out.at[i], states.at[side, i], state_send, state_recv.at[i], partner
            ).start()

    @pl.loop(0, half // 2)
    def _(j):
        for i in (2 * j, 2 * j + 1):
            state, decay = local_state(side * half + i)
            states[side, i] = state
            decays[side, i] = decay

    @pl.loop(0, half)
    def _(j):
        for h in (2 * j, 2 * j + 1):
            cut = pair_rows(h, KEY_WIDTH)
            wide = pair_rows(h, DV)
            scores = lax.dot_general(
                lifted[:, cut], lowered[:, cut], (((1,), (1,)), ((), ())),
                preferred_element_type=jnp.float32,
            )
            scores = jnp.where(causal, scores, 0.0).astype(jnp.bfloat16)
            inside[:, wide] = jnp.dot(scores, v_ref[:, wide], preferred_element_type=jnp.float32)

    def finish(h, state):
        wide = pair_rows(h, DV)
        mixed = inside[:, wide] + lax.dot_general(
            reached[:, pair_rows(h, KEY_WIDTH)], state, (((1,), (1,)), ((), ())),
            preferred_element_type=jnp.float32,
        )
        own_heads[h] = rms_scale(mixed, gain_ref[:, wide]).astype(jnp.bfloat16)
        for k in range(1, ys):
            remote(
                own_heads.at[h], peer_heads.at[k - 1, h],
                head_send.at[k - 1], head_recv.at[k - 1, h], peer_y(k),
            ).start()

    def finish_crossed(i):
        pltpu.make_async_copy(crossed.at[i], crossed.at[i], cross_recv.at[i]).wait()
        finish((1 - side) * half + i, crossed[i])

    lag = jnp.maximum(3, half - 2 * pair)

    @pl.loop(0, half)
    def _(i):
        pltpu.make_async_copy(decays_out.at[i], decays_out.at[i], decay_recv.at[i]).wait()
        pltpu.make_async_copy(states_out.at[i], states_out.at[i], state_recv.at[i]).wait()

        @pl.when(pair > 0)
        def _():
            pltpu.make_async_copy(onward.at[i], onward.at[i], chain_recv.at[i]).wait()

        middle = entering[0, i].astype(jnp.float32) * decays[0, i] + states[0, i].astype(jnp.float32)
        entering[1, i] = middle.astype(jnp.bfloat16)
        onward[i] = (middle * decays[1, i] + states[1, i].astype(jnp.float32)).astype(jnp.bfloat16)

        @pl.when(pair < pairs - 1)
        def _():
            remote(
                onward.at[i], entering.at[0, i], chain_send, chain_recv.at[i], (sp + 2, dp)
            ).start()

        remote(
            entering.at[1 - side, i], crossed.at[i], cross_send, cross_recv.at[i], partner
        ).start()
        finish(side * half + i, entering[side, i])

        @pl.when(i >= lag)
        def _():
            finish_crossed(i - lag)

    @pl.loop(half - lag, half)
    def _(i):
        finish_crossed(i)

    loads[5].wait()
    w_copy.wait_recv()

    def project(head_of, ready):
        total = None
        for h in range(heads):
            ready(h)
            wide = pl.ds(h * DV, DV)
            part = [
                jnp.dot(head_of(h), w_buf[c, wide, :], preferred_element_type=jnp.float32)
                for c in range(2)
            ]
            total = part if total is None else [a + b for a, b in zip(total, part)]
        return jnp.concatenate(total, axis=1).astype(jnp.bfloat16)

    for k in range(1, ys):
        def ready(h, k=k):
            pltpu.make_async_copy(
                peer_heads.at[k - 1, h], peer_heads.at[k - 1, h], head_recv.at[k - 1, h]
            ).wait()

        proj_out[k - 1] = project(lambda h, k=k: peer_heads[k - 1, h], ready)
        back = (sp, lax.rem(y - k + ys, ys) * 2 + core)
        remote(proj_out.at[k - 1], proj.at[y], proj_send, proj_recv, back).start()
    proj[y] = project(lambda h: own_heads[h], lambda h: None)
    loads[4].wait()
    arrived = proj.at[pl.ds(0, ys - 1)]
    pltpu.make_async_copy(arrived, arrived, proj_recv).wait()
    projected = jnp.concatenate([proj[i] for i in range(ys)], axis=1).astype(jnp.float32)
    residual = stream_ref[...].astype(jnp.float32) + rms_scale(projected, branch_ref[...])
    residual = residual.astype(jnp.bfloat16)
    residuals[...] = residual
    inputs = rms_scale(residual.astype(jnp.float32), pre_ref[...]).astype(jnp.bfloat16)
    segments = D // LANES
    tokens[...] = inputs.reshape(rows, segments, LANES)
    for copy in tables:
        copy.wait()

    def group_of(step):
        across = lax.rem(plane + step // 2 * 2, PLANES)
        return across + lax.rem(step, 2) * (1 - 2 * lax.rem(across, 2))

    def block(ref, peer):
        return ref.at[peer]

    @pl.loop(0, total)
    def _(i):
        group = group_of(lax.rem(i // per + 2, PLANES))
        peer = group * per + lax.rem(place + lax.rem(i, per), per)
        for r in range(cap):
            outgoing[peer, r] = tokens[jnp.clip(sources[0, peer * cap + r], 0, rows - 1)]

        @pl.when(peer != me)
        def _():
            remote(
                block(outgoing, peer), block(arrivals, me), row_send, row_recv.at[plane],
                where_is(peer),
            ).start()

        @pl.when(peer == me)
        def _():
            pltpu.make_async_copy(
                block(outgoing, me), block(arrivals, me), row_recv.at[plane]
            ).start()

    for copy in weights:
        copy.wait()

    @pl.loop(0, PLANES)
    def _(step):
        group = group_of(step)
        base = group * per
        batch = pl.ds(base, per)
        pltpu.make_async_copy(arrivals.at[batch], arrivals.at[batch], row_recv.at[group]).wait()
        x = arrivals[batch].reshape(per * cap, D)
        gate_part = jnp.dot(x, gate_w[...], preferred_element_type=jnp.float32)
        up_part = jnp.dot(x, up_w[...], preferred_element_type=jnp.float32)
        hidden = (jax.nn.silu(gate_part) * up_part).astype(jnp.bfloat16)
        result = jnp.dot(hidden, down_w[...], preferred_element_type=jnp.float32)
        results[batch] = result.astype(jnp.bfloat16).reshape(per, cap, segments, LANES)

        @pl.loop(0, per)
        def _(j):
            peer = base + lax.rem(place + j, per)

            @pl.when(peer != me)
            def _():
                remote(
                    block(results, peer), block(returned, me), back_send, back_recv,
                    where_is(peer),
                ).start()

            @pl.when(peer == me)
            def _():
                pltpu.make_async_copy(
                    block(results, me), block(returned, me), back_recv
                ).start()

    pltpu.make_async_copy(returned, returned, back_recv).wait()

    @pl.loop(0, rows // 8)
    def _(i):
        for t in range(8):
            at = i * 8 + t
            rows_of = [
                returned[
                    jnp.clip(slots[j, at], 0, total - 1), jnp.clip(slots[TOP + j, at], 0, cap - 1)
                ].astype(jnp.float32)
                for j in range(TOP)
            ]
            combined[at] = rows_of[0] * shares[0, at] + rows_of[1] * shares[1, at]

    routed = rms_scale(combined[...].reshape(rows, D), post_ref[...])
    out_ref[...] = (residuals[...].astype(jnp.float32) + routed).astype(jnp.bfloat16)

    others = pl.ds(0, total - 1)
    pltpu.make_async_copy(outgoing.at[others], outgoing.at[others], row_send).wait()
    pltpu.make_async_copy(results.at[others], results.at[others], back_send).wait()

    sent = extras.at[pl.ds(0, sp_count - 1)]
    pltpu.make_async_copy(sent, sent, extra_send).wait()
    pltpu.make_async_copy(states_out, states_out, state_send).wait()
    pltpu.make_async_copy(decays_out, decays_out, decay_send).wait()
    w_copy.wait_send()
    pltpu.make_async_copy(crossed, crossed, cross_send).wait()

    @pl.when(pair < pairs - 1)
    def _():
        pltpu.make_async_copy(onward, onward, chain_send).wait()

    for k in range(1, ys):
        pltpu.make_async_copy(own_heads, own_heads, head_send.at[k - 1]).wait()
    pltpu.make_async_copy(proj_out, proj_out, proj_send).wait()


def layer(
    query, key, value, gate, stream, weight, gate_weight, up_weight, down_weight,
    extra, gain, branch_gain, pre_gain, post_gain, chosen, logits,
):
    rows, width = query.shape
    heads = width // KEY_WIDTH
    half = heads // 2
    sp_count, dp_count = lax.axis_size("sp"), lax.axis_size("dp")
    ys = dp_count // 2
    total = sp_count * dp_count
    cols = weight.shape[1]
    cap = max(2, 5 * rows * TOP // (3 * total))
    bf16, f32, i32 = jnp.bfloat16, jnp.float32, jnp.int32
    vmem = pl.BlockSpec(memory_space=pltpu.VMEM)
    anywhere = pl.BlockSpec(memory_space=pl.ANY)
    state = (DV, KEY_WIDTH)
    table = (1, -(-total * cap // LANES) * LANES)
    units = pltpu.VMEM((total, cap, D // LANES, LANES), bf16)
    dma = pltpu.SemaphoreType.DMA
    return pl.pallas_call(
        layer_kernel,
        in_specs=[anywhere] * 9 + [vmem] * 7,
        out_specs=vmem,
        out_shape=jax.ShapeDtypeStruct((rows, D), bf16),
        scratch_shapes=[
            pltpu.VMEM((rows, width), bf16),
            pltpu.VMEM((rows, width), bf16),
            pltpu.VMEM(value.shape, bf16),
            pltpu.VMEM((rows, width), bf16),
            pltpu.VMEM((rows, D), bf16),
            pltpu.VMEM((2,) + weight.shape, bf16),
            pltpu.VMEM((sp_count, extra.shape[0], rows), f32),
            pltpu.VMEM((rows, width), f32),
            pltpu.VMEM((rows, width), bf16),
            pltpu.VMEM((rows, width), bf16),
            pltpu.VMEM((rows, width), bf16),
            pltpu.VMEM(value.shape, f32),
            pltpu.VMEM((half,) + state, bf16),
            pltpu.VMEM((2, half) + state, bf16),
            pltpu.VMEM((half, 1, KEY_WIDTH), f32),
            pltpu.VMEM((2, half, 1, KEY_WIDTH), f32),
            pltpu.VMEM((2, half) + state, bf16),
            pltpu.VMEM((half,) + state, bf16),
            pltpu.VMEM((half,) + state, bf16),
            pltpu.VMEM((heads, rows, DV), bf16),
            pltpu.VMEM((ys - 1, heads, rows, DV), bf16),
            pltpu.VMEM((ys - 1, rows, 2 * cols), bf16),
            pltpu.VMEM((ys, rows, 2 * cols), bf16),
            dma((6,)), dma((2,)), dma, dma, dma, dma((half,)), dma, dma((half,)),
            dma, dma((half,)), dma, dma((half,)), dma((ys - 1,)), dma((ys - 1, heads)), dma, dma,
            pltpu.VMEM((rows, D), bf16),
            pltpu.VMEM((rows, D // LANES, LANES), bf16),
            units, units, units, units,
            pltpu.VMEM((rows, D // LANES, LANES), f32),
            *[pltpu.VMEM(w.shape[1:], bf16) for w in (gate_weight, up_weight, down_weight)],
            pltpu.VMEM((2 * TOP, rows), i32),
            pltpu.VMEM(table, i32),
            pltpu.VMEM((TOP, rows), f32),
            pltpu.SMEM((2 * TOP, rows), i32),
            pltpu.SMEM(table, i32),
            pltpu.SMEM((TOP, rows), f32),
            dma((3,)), dma((3,)), dma, dma((PLANES,)), dma, dma,
        ],
        compiler_params=pltpu.CompilerParams(
            collective_id=0, has_side_effects=True, vmem_limit_bytes=60 * 1024 * 1024
        ),
        name="layer",
    )(
        query, key, value, gate, stream, weight, gate_weight, up_weight, down_weight,
        extra, gain.reshape(1, -1), branch_gain.reshape(1, -1), pre_gain.reshape(1, -1),
        post_gain.reshape(1, -1), chosen, logits,
    )


def shards(
    skip_stream_entering,
    mapped_probe_matrix,
    mapped_lookup_matrix,
    mapped_content_matrix,
    retention_preactivation,
    extra_shrinkage,
    attention_group_scale,
    final_projection_matrix,
    blender_branch_scale,
    specialist_prenormal_scale,
    specialist_switch_matrix,
    specialist_expand_matrix,
    specialist_contract_matrix,
    specialist_branch_scale,
    assigned_specialists,
    dispatcher_logits,
):
    out = layer(
        mapped_probe_matrix[0],
        mapped_lookup_matrix[0],
        mapped_content_matrix[0],
        retention_preactivation[0],
        skip_stream_entering[0],
        final_projection_matrix,
        specialist_switch_matrix,
        specialist_expand_matrix,
        specialist_contract_matrix,
        extra_shrinkage[0],
        attention_group_scale,
        blender_branch_scale,
        specialist_prenormal_scale,
        specialist_branch_scale,
        jnp.transpose(assigned_specialists[0]),
        jnp.transpose(dispatcher_logits[0]),
    )
    return out[None]


def solution(mesh):
    return jax.shard_map(
        shards,
        mesh=mesh,
        in_specs=(
            P("dp", "sp", None),
            P("dp", "sp", None),
            P("dp", "sp", None),
            P("dp", "sp", None),
            P("dp", "sp", None),
            P("dp", "sp", None),
            P(),
            P(None, "dp"),
            P(),
            P(),
            P(("sp", "dp"), None, None),
            P(("sp", "dp"), None, None),
            P(("sp", "dp"), None, None),
            P(),
            P("dp", "sp", None),
            P("dp", "sp", None),
        ),
        out_specs=P("dp", "sp", None),
        check_vma=False,
    )
```

```python
import functools

import jax
import jax.numpy as jnp
from jax import lax
from jax.experimental import pallas as pl
from jax.experimental.pallas import tpu as pltpu
from jax.sharding import PartitionSpec as P

D = 2048
KEY_WIDTH = 128
DV = 256
TOP = 2
BLOCK = 64


epsilon = 1e-06
softness_factor = 16.0


def rms_scale(values, gain):
    mean_square = jnp.mean(values * values, axis=-1, keepdims=True)
    return values * lax.rsqrt(mean_square + epsilon) * gain


CHUNKS = 4
LANES = 128
MESH = pl.DeviceIdType.MESH


def pair_rows(h, width):
    return pl.ds(pl.multiple_of(h * width, width), width)


def layer_kernel(
    q_hbm, k_hbm, v_hbm, g_hbm, stream_hbm, w_hbm, gate_hbm, up_hbm, down_hbm,
    extra_ref, gain_ref, branch_ref, pre_ref, post_ref, chosen_ref, logits_ref, out_ref,
    q_ref, k_ref, v_ref, g_ref, stream_ref, w_buf, extras, within, lifted, lowered, reached, inside,
    states_out, states, decays_out, decays, entering, onward, crossed, own_heads, peer_heads,
    proj_out, proj,
    load_sem, w_sem, extra_send, extra_recv, state_send, state_recv, decay_send, decay_recv,
    chain_send, chain_recv, cross_send, cross_recv, head_send, head_recv, proj_send, proj_recv,
    residuals, tokens, far_tokens, outgoing, arrivals, results, returned, sums_out, sums_in, combined,
    gate_w, up_w, down_w, far_chosen, far_logits,
    route_rows, source_rows, share_rows, slots, sources, shares,
    weight_sem, route_sem, far_send, far_recv, token_send, token_recv, row_send, row_recv,
    back_send, back_recv, sum_send, sum_recv,
):
    sp_count, dp_count = lax.axis_size("sp"), lax.axis_size("dp")
    sp, dp = lax.axis_index("sp"), lax.axis_index("dp")
    pair, side = sp // 2, lax.rem(sp, 2)
    pairs = sp_count // 2
    y, core = dp // 2, lax.rem(dp, 2)
    ys = dp_count // 2
    rows = q_ref.shape[0]
    heads = q_ref.shape[1] // KEY_WIDTH
    half = heads // 2
    own = extra_ref.shape[0]
    cols = w_hbm.shape[1]
    partner = (sp + 1 - 2 * side, dp)
    twin = (sp, dp + 1 - 2 * core)

    def remote(src, dst, send, recv, where):
        return pltpu.make_async_remote_copy(
            src_ref=src, dst_ref=dst, send_sem=send, recv_sem=recv,
            device_id=where, device_id_type=MESH,
        )

    def peer_y(k):
        return (sp, lax.rem(y + k, ys) * 2 + core)

    loads = [
        pltpu.make_async_copy(src, dst, load_sem.at[i])
        for i, (src, dst) in enumerate(
            ((g_hbm, g_ref), (k_hbm, k_ref), (v_hbm, v_ref), (q_hbm, q_ref),
             (stream_hbm, stream_ref), (w_hbm, w_buf.at[core]))
        )
    ]
    for copy in loads:
        copy.start()

    total = sp_count * dp_count
    me = sp * dp_count + dp
    cap = outgoing.shape[3]
    near = total // 2
    per = near // 2
    side_half, place = me // near, lax.rem(me, near)
    mirror = lax.rem(me + near, total)

    def where_is(peer):
        return (peer // dp_count, lax.rem(peer, dp_count))

    barrier = pltpu.get_barrier_semaphore()

    @pl.loop(1, total)
    def _(i):
        peer = lax.rem(me + i, total)
        pl.semaphore_signal(barrier, inc=1, device_id=where_is(peer), device_id_type=MESH)

    row = lax.broadcasted_iota(jnp.int32, (rows, rows), 0)
    col = lax.broadcasted_iota(jnp.int32, (rows, rows), 1)
    causal = row >= col
    ones = jnp.where(causal, 1.0, 0.0).astype(jnp.bfloat16)
    ones = jnp.concatenate([ones, ones], axis=1)

    def build_tables(t, picked, scores):
        expert = lax.broadcasted_iota(jnp.int32, (near, rows), 0)
        picks = [picked[j : j + 1] - side_half * near for j in range(TOP)]
        named = functools.reduce(jnp.logical_or, [expert == pick for pick in picks])
        before = jnp.dot(
            jnp.where(named, 1.0, 0.0).astype(jnp.bfloat16),
            jnp.where(row < col, 1.0, 0.0).astype(jnp.bfloat16),
            preferred_element_type=jnp.float32,
        )
        spot = lax.broadcasted_iota(jnp.int32, (rows, source_rows.shape[2]), 1).astype(jnp.float32)
        token = lax.broadcasted_iota(jnp.int32, spot.shape, 0).astype(jnp.float32)
        source = jnp.zeros(spot.shape, jnp.float32)
        score = sum(scores[j : j + 1] for j in range(TOP))
        for j, pick in enumerate(picks):
            here = jnp.logical_and(pick >= 0, pick < near)
            rank = jnp.sum(jnp.where(expert == pick, before, 0.0), axis=0, keepdims=True)
            slot = jnp.where(here, pick.astype(jnp.float32) * cap + rank, -1.0)
            route_rows[t, j : j + 1] = jnp.clip(pick, 0, near - 1)
            route_rows[t, TOP + j : TOP + j + 1] = jnp.clip(rank.astype(jnp.int32), 0, cap - 1)
            share_rows[t, j : j + 1] = jnp.where(here, scores[j : j + 1] / score, 0.0)
            upright = jnp.sum(jnp.where(row == col, slot, 0.0), axis=1, keepdims=True)
            source = source + jnp.where(spot == upright, token, 0.0)
        source = jnp.sum(source, axis=0, keepdims=True).astype(jnp.int32)
        source_rows[t] = jnp.clip(source, 0, rows - 1)

    build_tables(0, chosen_ref[...], logits_ref[...])
    loads[0].wait()

    @pl.loop(0, half)
    def _(j):
        cut = pair_rows(j, 2 * KEY_WIDTH)
        g = g_ref[:, cut].astype(jnp.float32)
        logs = (jnp.minimum(g, 0.0) - jnp.log(1.0 + jnp.exp(-jnp.abs(g)))) / softness_factor
        high = logs.astype(jnp.bfloat16)
        low = (logs - high.astype(jnp.float32)).astype(jnp.bfloat16)
        within[:, cut] = jnp.dot(
            ones, jnp.concatenate([high, low], axis=0), preferred_element_type=jnp.float32
        )

    pl.semaphore_wait(barrier, total - 1)
    far_copies = [
        remote(src, dst, far_send.at[i], far_recv.at[i], where_is(mirror))
        for i, (src, dst) in enumerate(((chosen_ref, far_chosen), (logits_ref, far_logits)))
    ]

    @pl.loop(1, sp_count)
    def _(i):
        peer = lax.rem(sp + i, sp_count)
        remote(
            extra_ref.at[:, pair_rows(peer, rows)], extras.at[sp], extra_send, extra_recv, (peer, dp)
        ).start()

    pltpu.make_async_copy(
        extra_ref.at[:, pair_rows(sp, rows)], extras.at[sp], extra_recv
    ).start()
    w_copy = remote(w_hbm, w_buf.at[core], w_sem.at[0], w_sem.at[1], twin)
    w_copy.start()
    for copy in far_copies:
        copy.start()

    @pl.when(pair == 0)
    def _():
        entering[0] = jnp.zeros(entering.shape[1:], entering.dtype)

    for copy in loads[1:4]:
        copy.wait()
    weights = [
        pltpu.make_async_copy(src.at[0], dst, weight_sem.at[i])
        for i, (src, dst) in enumerate(
            ((gate_hbm, gate_w), (up_hbm, up_w), (down_hbm, down_w))
        )
    ]
    for copy in weights:
        copy.start()
    pltpu.make_async_copy(extras, extras, extra_recv).wait()

    def local_state(h):
        cut = pair_rows(h, KEY_WIDTH)
        extra = jnp.sum(
            jnp.where(causal, extras[h // own, pl.ds(lax.rem(h, own), 1)], 0.0),
            axis=1, keepdims=True,
        )
        b = within[:, cut] + extra
        middle = b[rows // 2 - 1 : rows // 2]
        end = b[rows - 1 : rows]
        up = jnp.exp(b - middle)
        down = jnp.exp(middle - b)
        q = q_ref[:, cut].astype(jnp.float32) * (KEY_WIDTH ** (-0.5)) * up
        k = k_ref[:, cut].astype(jnp.float32) * down
        lifted[:, cut] = q.astype(jnp.bfloat16)
        lowered[:, cut] = k.astype(jnp.bfloat16)
        reached[:, cut] = (q * jnp.exp(middle)).astype(jnp.bfloat16)
        carried = (k * jnp.exp(end - middle)).astype(jnp.bfloat16)
        state = lax.dot_general(
            v_ref[:, pair_rows(h, DV)], carried, (((0,), (0,)), ((), ())),
            preferred_element_type=jnp.float32,
        )
        return state.astype(jnp.bfloat16), jnp.exp(end)

    @pl.loop(0, half // 2)
    def _(j):
        for i in (2 * j, 2 * j + 1):
            state, decay = local_state((1 - side) * half + i)
            states_out[i] = state
            decays_out[i] = decay
        for i in (2 * j, 2 * j + 1):
            remote(
                decays_out.at[i], decays.at[side, i], decay_send, decay_recv.at[i], partner
            ).start()
            remote(
                states_out.at[i], states.at[side, i], state_send, state_recv.at[i], partner
            ).start()

    @pl.loop(0, half // 2)
    def _(j):
        for i in (2 * j, 2 * j + 1):
            state, decay = local_state(side * half + i)
            states[side, i] = state
            decays[side, i] = decay

    @pl.loop(0, half)
    def _(j):
        for h in (2 * j, 2 * j + 1):
            cut = pair_rows(h, KEY_WIDTH)
            wide = pair_rows(h, DV)
            scores = lax.dot_general(
                lifted[:, cut], lowered[:, cut], (((1,), (1,)), ((), ())),
                preferred_element_type=jnp.float32,
            )
            scores = jnp.where(causal, scores, 0.0).astype(jnp.bfloat16)
            inside[:, wide] = jnp.dot(scores, v_ref[:, wide], preferred_element_type=jnp.float32)

    def finish(h, state):
        wide = pair_rows(h, DV)
        mixed = inside[:, wide] + lax.dot_general(
            reached[:, pair_rows(h, KEY_WIDTH)], state, (((1,), (1,)), ((), ())),
            preferred_element_type=jnp.float32,
        )
        own_heads[h] = rms_scale(mixed, gain_ref[:, wide]).astype(jnp.bfloat16)
        for k in range(1, ys):
            remote(
                own_heads.at[h], peer_heads.at[k - 1, h],
                head_send.at[k - 1], head_recv.at[k - 1, h], peer_y(k),
            ).start()

    def finish_crossed(i):
        pltpu.make_async_copy(crossed.at[i], crossed.at[i], cross_recv.at[i]).wait()
        finish((1 - side) * half + i, crossed[i])

    for copy in far_copies:
        copy.wait_recv()
    build_tables(1, far_chosen[...], far_logits[...])
    tables = [
        pltpu.make_async_copy(src, dst, route_sem.at[i])
        for i, (src, dst) in enumerate(
            ((route_rows, slots), (source_rows, sources), (share_rows, shares))
        )
    ]
    for copy in tables:
        copy.start()
    lag = jnp.maximum(3, half - 2 * pair)

    @pl.loop(0, half)
    def _(i):
        pltpu.make_async_copy(decays_out.at[i], decays_out.at[i], decay_recv.at[i]).wait()
        pltpu.make_async_copy(states_out.at[i], states_out.at[i], state_recv.at[i]).wait()

        @pl.when(pair > 0)
        def _():
            pltpu.make_async_copy(onward.at[i], onward.at[i], chain_recv.at[i]).wait()

        middle = entering[0, i].astype(jnp.float32) * decays[0, i] + states[0, i].astype(jnp.float32)
        entering[1, i] = middle.astype(jnp.bfloat16)
        onward[i] = (middle * decays[1, i] + states[1, i].astype(jnp.float32)).astype(jnp.bfloat16)

        @pl.when(pair < pairs - 1)
        def _():
            remote(
                onward.at[i], entering.at[0, i], chain_send, chain_recv.at[i], (sp + 2, dp)
            ).start()

        remote(
            entering.at[1 - side, i], crossed.at[i], cross_send, cross_recv.at[i], partner
        ).start()
        finish(side * half + i, entering[side, i])

        @pl.when(i >= lag)
        def _():
            finish_crossed(i - lag)

    @pl.loop(half - lag, half)
    def _(i):
        finish_crossed(i)

    loads[5].wait()
    w_copy.wait_recv()

    def project(head_of, ready):
        total = None
        for h in range(heads):
            ready(h)
            wide = pl.ds(h * DV, DV)
            part = [
                jnp.dot(head_of(h), w_buf[c, wide, :], preferred_element_type=jnp.float32)
                for c in range(2)
            ]
            total = part if total is None else [a + b for a, b in zip(total, part)]
        return jnp.concatenate(total, axis=1).astype(jnp.bfloat16)

    for k in range(1, ys):
        def ready(h, k=k):
            pltpu.make_async_copy(
                peer_heads.at[k - 1, h], peer_heads.at[k - 1, h], head_recv.at[k - 1, h]
            ).wait()

        proj_out[k - 1] = project(lambda h, k=k: peer_heads[k - 1, h], ready)
        back = (sp, lax.rem(y - k + ys, ys) * 2 + core)
        remote(proj_out.at[k - 1], proj.at[y], proj_send, proj_recv, back).start()
    proj[y] = project(lambda h: own_heads[h], lambda h: None)
    loads[4].wait()
    arrived = proj.at[pl.ds(0, ys - 1)]
    pltpu.make_async_copy(arrived, arrived, proj_recv).wait()
    projected = jnp.concatenate([proj[i] for i in range(ys)], axis=1).astype(jnp.float32)
    residual = stream_ref[...].astype(jnp.float32) + rms_scale(projected, branch_ref[...])
    residual = residual.astype(jnp.bfloat16)
    residuals[...] = residual
    inputs = rms_scale(residual.astype(jnp.float32), pre_ref[...]).astype(jnp.bfloat16)
    piece = D // CHUNKS
    segments = piece // LANES
    for c in range(CHUNKS):
        tokens[c] = inputs[:, c * piece : (c + 1) * piece].reshape(rows, segments, LANES)
    for copy in tables:
        copy.wait()

    def neighbour(i):
        first = lax.rem(place // per + 1 + i // per, 2)
        return first * per + lax.rem(place + lax.rem(i, per), per)

    def exchange(src, dst, send, recv, peer):
        where = side_half * near + peer

        @pl.when(peer != place)
        def _():
            remote(src.at[peer], dst.at[place], send, recv, where_is(where)).start()

        @pl.when(peer == place)
        def _():
            pltpu.make_async_copy(src.at[place], dst.at[place], recv).start()

    def dispatch(t, c, start, stop):
        @pl.loop(start, stop)
        def _(i):
            peer = neighbour(i)
            for r in range(cap):
                source = jnp.clip(sources[t, 0, peer * cap + r], 0, rows - 1)
                outgoing[t, c, peer, r] = far_tokens[c][source] if t else tokens[c, source]
            exchange(outgoing.at[t, c], arrivals.at[t, c], row_send, row_recv.at[t, c], peer)

    def send_tokens():
        for c in range(CHUNKS):
            remote(
                tokens.at[c], far_tokens[c], token_send, token_recv.at[c], where_is(mirror)
            ).start()

    inner = side_half + place // per == 1

    @pl.when(inner)
    def _():
        send_tokens()

    for c in range(CHUNKS):
        dispatch(0, c, 0, per)

    @pl.when(jnp.logical_not(inner))
    def _():
        send_tokens()

    for c in range(CHUNKS):
        dispatch(0, c, per, near)

    def await_rows(t, c):
        pltpu.make_async_copy(arrivals.at[t, c], arrivals.at[t, c], row_recv.at[t, c]).wait()

    def answer(t, c):
        @pl.loop(0, near)
        def _(i):
            exchange(
                results.at[t, c], returned[t][c], back_send, back_recv.at[t, c], neighbour(i)
            )

    def expert_rows(t):
        gate_part, up_part = None, None
        for c in range(CHUNKS):
            await_rows(t, c)
            x = arrivals[t, c].reshape(near * cap, piece)
            cut = slice(c * piece, (c + 1) * piece)
            g = jnp.dot(x, gate_w[cut, :], preferred_element_type=jnp.float32)
            u = jnp.dot(x, up_w[cut, :], preferred_element_type=jnp.float32)
            gate_part = g if c == 0 else gate_part + g
            up_part = u if c == 0 else up_part + u
        hidden = (jax.nn.silu(gate_part) * up_part).astype(jnp.bfloat16)
        for c in range(CHUNKS):
            result = jnp.dot(
                hidden, down_w[:, c * piece : (c + 1) * piece], preferred_element_type=jnp.float32
            )
            results[t, c] = result.astype(jnp.bfloat16).reshape(near, cap, segments, LANES)
            if t == 1:
                answer(t, c)

    def token_sums(t, c, store):
        pltpu.make_async_copy(returned[t][c], returned[t][c], back_recv.at[t, c]).wait()

        @pl.loop(0, rows // 8)
        def _(i):
            for k in range(8):
                at = i * 8 + k
                parts = [
                    returned[t][c][
                        jnp.clip(slots[t, j, at], 0, near - 1),
                        jnp.clip(slots[t, TOP + j, at], 0, cap - 1),
                    ].astype(jnp.float32) * shares[t, j, at]
                    for j in range(TOP)
                ]
                store(at, sum(parts))

    for copy in weights:
        copy.wait()
    for c in range(CHUNKS):
        pltpu.make_async_copy(far_tokens[c], far_tokens[c], token_recv.at[c]).wait()
        dispatch(1, c, 0, near)
        if c == CHUNKS // 2 - 1:
            expert_rows(0)
    expert_rows(1)
    for c in range(CHUNKS):
        answer(0, c)
    for c in range(CHUNKS):
        def store_far(at, value, c=c):
            sums_out[c, at] = value.astype(jnp.bfloat16)

        token_sums(1, c, store_far)
        remote(
            sums_out.at[c], sums_in.at[c], sum_send, sum_recv.at[c], where_is(mirror)
        ).start()
    for c in range(CHUNKS):
        def store_own(at, value, c=c):
            combined[c, at] = value

        token_sums(0, c, store_own)
    whole = []
    for c in range(CHUNKS):
        pltpu.make_async_copy(sums_in.at[c], sums_in.at[c], sum_recv.at[c]).wait()
        value = combined[c] + sums_in[c].astype(jnp.float32)
        whole.append(value.reshape(rows, piece))
    routed = rms_scale(jnp.concatenate(whole, axis=1), post_ref[...])
    out_ref[...] = (residuals[...].astype(jnp.float32) + routed).astype(jnp.bfloat16)

    for copy in far_copies:
        copy.wait_send()
    pltpu.make_async_copy(tokens, tokens, token_send).wait()
    pltpu.make_async_copy(sums_out, sums_out, sum_send).wait()
    others = pl.ds(0, near - 1)
    for ref, sem in ((outgoing, row_send), (results, back_send)):
        done = ref.at[:, :, others]
        pltpu.make_async_copy(done, done, sem).wait()

    sent = extras.at[pl.ds(0, sp_count - 1)]
    pltpu.make_async_copy(sent, sent, extra_send).wait()
    pltpu.make_async_copy(states_out, states_out, state_send).wait()
    pltpu.make_async_copy(decays_out, decays_out, decay_send).wait()
    w_copy.wait_send()
    pltpu.make_async_copy(crossed, crossed, cross_send).wait()

    @pl.when(pair < pairs - 1)
    def _():
        pltpu.make_async_copy(onward, onward, chain_send).wait()

    for k in range(1, ys):
        pltpu.make_async_copy(own_heads, own_heads, head_send.at[k - 1]).wait()
    pltpu.make_async_copy(proj_out, proj_out, proj_send).wait()


def layer(
    query, key, value, gate, stream, weight, gate_weight, up_weight, down_weight,
    extra, gain, branch_gain, pre_gain, post_gain, chosen, logits,
):
    rows, width = query.shape
    heads = width // KEY_WIDTH
    half = heads // 2
    sp_count, dp_count = lax.axis_size("sp"), lax.axis_size("dp")
    ys = dp_count // 2
    total = sp_count * dp_count
    cols = weight.shape[1]
    cap = max(2, 5 * rows * TOP // (3 * total))
    bf16, f32, i32 = jnp.bfloat16, jnp.float32, jnp.int32
    vmem = pl.BlockSpec(memory_space=pltpu.VMEM)
    anywhere = pl.BlockSpec(memory_space=pl.ANY)
    state = (DV, KEY_WIDTH)
    near = total // 2
    table = (2, 1, -(-near * cap // LANES) * LANES)
    segments = D // CHUNKS // LANES
    units = pltpu.VMEM((2, CHUNKS, near, cap, segments, LANES), bf16)
    unit = pltpu.VMEM((near, cap, segments, LANES), bf16)
    sums = pltpu.VMEM((CHUNKS, rows, segments, LANES), bf16)
    dma = pltpu.SemaphoreType.DMA
    return pl.pallas_call(
        layer_kernel,
        in_specs=[anywhere] * 9 + [vmem] * 7,
        out_specs=vmem,
        out_shape=jax.ShapeDtypeStruct((rows, D), bf16),
        scratch_shapes=[
            pltpu.VMEM((rows, width), bf16),
            pltpu.VMEM((rows, width), bf16),
            pltpu.VMEM(value.shape, bf16),
            pltpu.VMEM((rows, width), bf16),
            pltpu.VMEM((rows, D), bf16),
            pltpu.VMEM((2,) + weight.shape, bf16),
            pltpu.VMEM((sp_count, extra.shape[0], rows), f32),
            pltpu.VMEM((rows, width), f32),
            pltpu.VMEM((rows, width), bf16),
            pltpu.VMEM((rows, width), bf16),
            pltpu.VMEM((rows, width), bf16),
            pltpu.VMEM(value.shape, f32),
            pltpu.VMEM((half,) + state, bf16),
            pltpu.VMEM((2, half) + state, bf16),
            pltpu.VMEM((half, 1, KEY_WIDTH), f32),
            pltpu.VMEM((2, half, 1, KEY_WIDTH), f32),
            pltpu.VMEM((2, half) + state, bf16),
            pltpu.VMEM((half,) + state, bf16),
            pltpu.VMEM((half,) + state, bf16),
            pltpu.VMEM((heads, rows, DV), bf16),
            pltpu.VMEM((ys - 1, heads, rows, DV), bf16),
            pltpu.VMEM((ys - 1, rows, 2 * cols), bf16),
            pltpu.VMEM((ys, rows, 2 * cols), bf16),
            dma((6,)), dma((2,)), dma, dma, dma, dma((half,)), dma, dma((half,)),
            dma, dma((half,)), dma, dma((half,)), dma((ys - 1,)), dma((ys - 1, heads)), dma, dma,
            pltpu.VMEM((rows, D), bf16),
            sums, [pltpu.VMEM((rows, segments, LANES), bf16)] * CHUNKS,
            units, units, units, [[unit] * CHUNKS] * 2, sums, sums,
            pltpu.VMEM((CHUNKS, rows, segments, LANES), f32),
            *[pltpu.VMEM(w.shape[1:], bf16) for w in (gate_weight, up_weight, down_weight)],
            pltpu.VMEM((TOP, rows), i32),
            pltpu.VMEM((TOP, rows), f32),
            pltpu.VMEM((2, 2 * TOP, rows), i32),
            pltpu.VMEM(table, i32),
            pltpu.VMEM((2, TOP, rows), f32),
            pltpu.SMEM((2, 2 * TOP, rows), i32),
            pltpu.SMEM(table, i32),
            pltpu.SMEM((2, TOP, rows), f32),
            dma((3,)), dma((3,)), dma((2,)), dma((2,)), dma, dma((CHUNKS,)), dma, dma((2, CHUNKS)),
            dma, dma((2, CHUNKS)), dma, dma((CHUNKS,)),
        ],
        compiler_params=pltpu.CompilerParams(
            collective_id=0, has_side_effects=True, vmem_limit_bytes=60 * 1024 * 1024
        ),
        name="layer",
    )(
        query, key, value, gate, stream, weight, gate_weight, up_weight, down_weight,
        extra, gain.reshape(1, -1), branch_gain.reshape(1, -1), pre_gain.reshape(1, -1),
        post_gain.reshape(1, -1), chosen, logits,
    )


def shards(
    skip_stream_entering,
    mapped_probe_matrix,
    mapped_lookup_matrix,
    mapped_content_matrix,
    retention_preactivation,
    extra_shrinkage,
    attention_group_scale,
    final_projection_matrix,
    blender_branch_scale,
    specialist_prenormal_scale,
    specialist_switch_matrix,
    specialist_expand_matrix,
    specialist_contract_matrix,
    specialist_branch_scale,
    assigned_specialists,
    dispatcher_logits,
):
    out = layer(
        mapped_probe_matrix[0],
        mapped_lookup_matrix[0],
        mapped_content_matrix[0],
        retention_preactivation[0],
        skip_stream_entering[0],
        final_projection_matrix,
        specialist_switch_matrix,
        specialist_expand_matrix,
        specialist_contract_matrix,
        extra_shrinkage[0],
        attention_group_scale,
        blender_branch_scale,
        specialist_prenormal_scale,
        specialist_branch_scale,
        jnp.transpose(assigned_specialists[0]),
        jnp.transpose(dispatcher_logits[0]),
    )
    return out[None]


def solution(mesh):
    return jax.shard_map(
        shards,
        mesh=mesh,
        in_specs=(
            P("dp", "sp", None),
            P("dp", "sp", None),
            P("dp", "sp", None),
            P("dp", "sp", None),
            P("dp", "sp", None),
            P("dp", "sp", None),
            P(),
            P(None, "dp"),
            P(),
            P(),
            P(("sp", "dp"), None, None),
            P(("sp", "dp"), None, None),
            P(("sp", "dp"), None, None),
            P(),
            P("dp", "sp", None),
            P("dp", "sp", None),
        ),
        out_specs=P("dp", "sp", None),
        check_vma=False,
    )
```

```python
import functools

import jax
import jax.numpy as jnp
from jax import lax
from jax.experimental import pallas as pl
from jax.experimental.pallas import tpu as pltpu
from jax.sharding import PartitionSpec as P

D = 2048
KEY_WIDTH = 128
DV = 256
TOP = 2
BLOCK = 64


epsilon = 1e-06
softness_factor = 16.0


def rms_scale(values, gain):
    mean_square = jnp.mean(values * values, axis=-1, keepdims=True)
    return values * lax.rsqrt(mean_square + epsilon) * gain


CHUNKS = 4
PARTS = 4
LANES = 128
MESH = pl.DeviceIdType.MESH


def pair_rows(h, width):
    return pl.ds(pl.multiple_of(h * width, width), width)


def layer_kernel(
    q_hbm, k_hbm, v_hbm, g_hbm, stream_hbm, w_hbm, gate_hbm, up_hbm, down_hbm,
    extra_ref, gain_ref, branch_ref, pre_ref, post_ref, chosen_ref, logits_ref, out_ref,
    q_ref, k_ref, v_ref, g_ref, stream_ref, w_buf, extras, within, lifted, lowered, reached, inside,
    states_out, states, decays_out, decays, entering, onward, crossed, own_heads, peer_heads,
    proj_out, proj,
    load_sem, w_sem, extra_send, extra_recv, state_send, state_recv, decay_send, decay_recv,
    chain_send, chain_recv, cross_send, cross_recv, head_send, head_recv, proj_send, proj_recv,
    residuals, tokens, far_tokens, outgoing, arrivals, results, returned, sums_out, sums_in, combined,
    gate_w, up_w, down_w, far_chosen, far_logits,
    route_rows, source_rows, share_rows, slots, sources, shares,
    weight_sem, route_sem, far_send, far_recv, token_send, token_recv, row_send, row_recv,
    back_send, back_recv, sum_send, sum_recv,
):
    sp_count, dp_count = lax.axis_size("sp"), lax.axis_size("dp")
    sp, dp = lax.axis_index("sp"), lax.axis_index("dp")
    pair, side = sp // 2, lax.rem(sp, 2)
    pairs = sp_count // 2
    y, core = dp // 2, lax.rem(dp, 2)
    ys = dp_count // 2
    rows = q_ref.shape[0]
    heads = q_ref.shape[1] // KEY_WIDTH
    half = heads // 2
    own = extra_ref.shape[0]
    cols = w_hbm.shape[1]
    partner = (sp + 1 - 2 * side, dp)
    twin = (sp, dp + 1 - 2 * core)

    def remote(src, dst, send, recv, where):
        return pltpu.make_async_remote_copy(
            src_ref=src, dst_ref=dst, send_sem=send, recv_sem=recv,
            device_id=where, device_id_type=MESH,
        )

    def peer_y(k):
        return (sp, lax.rem(y + k, ys) * 2 + core)

    loads = [
        pltpu.make_async_copy(src, dst, load_sem.at[i])
        for i, (src, dst) in enumerate(
            ((g_hbm, g_ref), (k_hbm, k_ref), (v_hbm, v_ref), (q_hbm, q_ref),
             (stream_hbm, stream_ref), (w_hbm, w_buf.at[core]))
        )
    ]
    for copy in loads:
        copy.start()

    total = sp_count * dp_count
    me = sp * dp_count + dp
    cap = outgoing.shape[3]
    near = total // 2
    per = near // 2
    side_half, place = me // near, lax.rem(me, near)
    mirror = lax.rem(me + near, total)

    def where_is(peer):
        return (peer // dp_count, lax.rem(peer, dp_count))

    barrier = pltpu.get_barrier_semaphore()

    @pl.loop(1, total)
    def _(i):
        peer = lax.rem(me + i, total)
        pl.semaphore_signal(barrier, inc=1, device_id=where_is(peer), device_id_type=MESH)

    row = lax.broadcasted_iota(jnp.int32, (rows, rows), 0)
    col = lax.broadcasted_iota(jnp.int32, (rows, rows), 1)
    causal = row >= col
    ones = jnp.where(causal, 1.0, 0.0).astype(jnp.bfloat16)
    ones = jnp.concatenate([ones, ones], axis=1)

    def build_tables(t, picked, scores):
        expert = lax.broadcasted_iota(jnp.int32, (near, rows), 0)
        picks = [picked[j : j + 1] - side_half * near for j in range(TOP)]
        named = functools.reduce(jnp.logical_or, [expert == pick for pick in picks])
        before = jnp.dot(
            jnp.where(named, 1.0, 0.0).astype(jnp.bfloat16),
            jnp.where(row < col, 1.0, 0.0).astype(jnp.bfloat16),
            preferred_element_type=jnp.float32,
        )
        spot = lax.broadcasted_iota(jnp.int32, (rows, source_rows.shape[2]), 1).astype(jnp.float32)
        token = lax.broadcasted_iota(jnp.int32, spot.shape, 0).astype(jnp.float32)
        source = jnp.zeros(spot.shape, jnp.float32)
        score = sum(scores[j : j + 1] for j in range(TOP))
        for j, pick in enumerate(picks):
            here = jnp.logical_and(pick >= 0, pick < near)
            rank = jnp.sum(jnp.where(expert == pick, before, 0.0), axis=0, keepdims=True)
            slot = jnp.where(here, pick.astype(jnp.float32) * cap + rank, -1.0)
            route_rows[t, j : j + 1] = jnp.clip(pick, 0, near - 1)
            route_rows[t, TOP + j : TOP + j + 1] = jnp.clip(rank.astype(jnp.int32), 0, cap - 1)
            share_rows[t, j : j + 1] = jnp.where(here, scores[j : j + 1] / score, 0.0)
            upright = jnp.sum(jnp.where(row == col, slot, 0.0), axis=1, keepdims=True)
            source = source + jnp.where(spot == upright, token, 0.0)
        source = jnp.sum(source, axis=0, keepdims=True).astype(jnp.int32)
        source_rows[t] = jnp.clip(source, 0, rows - 1)

    build_tables(0, chosen_ref[...], logits_ref[...])
    loads[0].wait()

    @pl.loop(0, half)
    def _(j):
        cut = pair_rows(j, 2 * KEY_WIDTH)
        g = g_ref[:, cut].astype(jnp.float32)
        logs = (jnp.minimum(g, 0.0) - jnp.log(1.0 + jnp.exp(-jnp.abs(g)))) / softness_factor
        high = logs.astype(jnp.bfloat16)
        low = (logs - high.astype(jnp.float32)).astype(jnp.bfloat16)
        within[:, cut] = jnp.dot(
            ones, jnp.concatenate([high, low], axis=0), preferred_element_type=jnp.float32
        )

    pl.semaphore_wait(barrier, total - 1)
    far_copies = [
        remote(src, dst, far_send.at[i], far_recv.at[i], where_is(mirror))
        for i, (src, dst) in enumerate(((chosen_ref, far_chosen), (logits_ref, far_logits)))
    ]

    @pl.loop(1, sp_count)
    def _(i):
        peer = lax.rem(sp + i, sp_count)
        remote(
            extra_ref.at[:, pair_rows(peer, rows)], extras.at[sp], extra_send, extra_recv, (peer, dp)
        ).start()

    pltpu.make_async_copy(
        extra_ref.at[:, pair_rows(sp, rows)], extras.at[sp], extra_recv
    ).start()
    w_copy = remote(w_hbm, w_buf.at[core], w_sem.at[0], w_sem.at[1], twin)
    w_copy.start()
    for copy in far_copies:
        copy.start()

    @pl.when(pair == 0)
    def _():
        entering[0] = jnp.zeros(entering.shape[1:], entering.dtype)

    for copy in loads[1:4]:
        copy.wait()
    weights = [
        pltpu.make_async_copy(src.at[0], dst, weight_sem.at[i])
        for i, (src, dst) in enumerate(
            ((gate_hbm, gate_w), (up_hbm, up_w), (down_hbm, down_w))
        )
    ]
    for copy in weights:
        copy.start()
    pltpu.make_async_copy(extras, extras, extra_recv).wait()

    def state_cut(part):
        return pl.ds(part * (DV // PARTS), DV // PARTS)

    def local_state(h):
        cut = pair_rows(h, KEY_WIDTH)
        extra = jnp.sum(
            jnp.where(causal, extras[h // own, pl.ds(lax.rem(h, own), 1)], 0.0),
            axis=1, keepdims=True,
        )
        b = within[:, cut] + extra
        middle = b[rows // 2 - 1 : rows // 2]
        end = b[rows - 1 : rows]
        up = jnp.exp(b - middle)
        down = jnp.exp(middle - b)
        q = q_ref[:, cut].astype(jnp.float32) * (KEY_WIDTH ** (-0.5)) * up
        k = k_ref[:, cut].astype(jnp.float32) * down
        lifted[:, cut] = q.astype(jnp.bfloat16)
        lowered[:, cut] = k.astype(jnp.bfloat16)
        reached[:, cut] = (q * jnp.exp(middle)).astype(jnp.bfloat16)
        carried = (k * jnp.exp(end - middle)).astype(jnp.bfloat16)
        state = lax.dot_general(
            v_ref[:, pair_rows(h, DV)], carried, (((0,), (0,)), ((), ())),
            preferred_element_type=jnp.float32,
        )
        return state.astype(jnp.bfloat16), jnp.exp(end)

    @pl.loop(0, half // 2)
    def _(j):
        for i in (2 * j, 2 * j + 1):
            state, decay = local_state((1 - side) * half + i)
            states_out[i] = state
            decays_out[i] = decay
        for i in (2 * j, 2 * j + 1):
            remote(
                decays_out.at[i], decays.at[side, i], decay_send, decay_recv.at[i], partner
            ).start()
            for part in range(PARTS):
                cut = state_cut(part)
                remote(
                    states_out.at[i, cut], states.at[side, i, cut],
                    state_send, state_recv.at[i, part], partner,
                ).start()

    @pl.loop(0, half // 2)
    def _(j):
        for i in (2 * j, 2 * j + 1):
            state, decay = local_state(side * half + i)
            states[side, i] = state
            decays[side, i] = decay

    @pl.loop(0, half)
    def _(j):
        for h in (2 * j, 2 * j + 1):
            cut = pair_rows(h, KEY_WIDTH)
            wide = pair_rows(h, DV)
            scores = lax.dot_general(
                lifted[:, cut], lowered[:, cut], (((1,), (1,)), ((), ())),
                preferred_element_type=jnp.float32,
            )
            scores = jnp.where(causal, scores, 0.0).astype(jnp.bfloat16)
            inside[:, wide] = jnp.dot(scores, v_ref[:, wide], preferred_element_type=jnp.float32)

    def finish(h, state):
        wide = pair_rows(h, DV)
        mixed = inside[:, wide] + lax.dot_general(
            reached[:, pair_rows(h, KEY_WIDTH)], state, (((1,), (1,)), ((), ())),
            preferred_element_type=jnp.float32,
        )
        own_heads[h] = rms_scale(mixed, gain_ref[:, wide]).astype(jnp.bfloat16)
        for k in range(1, ys):
            remote(
                own_heads.at[h], peer_heads.at[k - 1, h],
                head_send.at[k - 1], head_recv.at[k - 1, h], peer_y(k),
            ).start()

    def finish_crossed(i):
        pltpu.make_async_copy(crossed.at[i], crossed.at[i], cross_recv.at[i]).wait()
        finish((1 - side) * half + i, crossed[i])

    for copy in far_copies:
        copy.wait_recv()
    build_tables(1, far_chosen[...], far_logits[...])
    tables = [
        pltpu.make_async_copy(src, dst, route_sem.at[i])
        for i, (src, dst) in enumerate(
            ((route_rows, slots), (source_rows, sources), (share_rows, shares))
        )
    ]
    for copy in tables:
        copy.start()
    lag = jnp.maximum(3, half - 2 * pair)

    @pl.loop(0, half)
    def _(i):
        pltpu.make_async_copy(decays_out.at[i], decays_out.at[i], decay_recv.at[i]).wait()
        for part in range(PARTS):
            cut = state_cut(part)
            there = states_out.at[i, cut]
            pltpu.make_async_copy(there, there, state_recv.at[i, part]).wait()

            @pl.when(pair > 0)
            def _():
                pltpu.make_async_copy(there, there, chain_recv.at[i, part]).wait()

            middle = entering[0, i, cut].astype(jnp.float32) * decays[0, i] + states[
                0, i, cut
            ].astype(jnp.float32)
            entering[1, i, cut] = middle.astype(jnp.bfloat16)
            onward[i, cut] = (
                middle * decays[1, i] + states[1, i, cut].astype(jnp.float32)
            ).astype(jnp.bfloat16)

            @pl.when(pair < pairs - 1)
            def _():
                remote(
                    onward.at[i, cut], entering.at[0, i, cut],
                    chain_send, chain_recv.at[i, part], (sp + 2, dp),
                ).start()

            remote(
                entering.at[1 - side, i, cut], crossed.at[i, cut],
                cross_send, cross_recv.at[i], partner,
            ).start()
        finish(side * half + i, entering[side, i])

        @pl.when(i >= lag)
        def _():
            finish_crossed(i - lag)

    @pl.loop(half - lag, half)
    def _(i):
        finish_crossed(i)

    loads[5].wait()
    w_copy.wait_recv()

    def project(head_of, ready):
        total = None
        for h in range(heads):
            ready(h)
            wide = pl.ds(h * DV, DV)
            part = [
                jnp.dot(head_of(h), w_buf[c, wide, :], preferred_element_type=jnp.float32)
                for c in range(2)
            ]
            total = part if total is None else [a + b for a, b in zip(total, part)]
        return jnp.concatenate(total, axis=1).astype(jnp.bfloat16)

    for k in range(1, ys):
        def ready(h, k=k):
            pltpu.make_async_copy(
                peer_heads.at[k - 1, h], peer_heads.at[k - 1, h], head_recv.at[k - 1, h]
            ).wait()

        proj_out[k - 1] = project(lambda h, k=k: peer_heads[k - 1, h], ready)
        back = (sp, lax.rem(y - k + ys, ys) * 2 + core)
        remote(proj_out.at[k - 1], proj.at[y], proj_send, proj_recv, back).start()
    proj[y] = project(lambda h: own_heads[h], lambda h: None)
    loads[4].wait()
    arrived = proj.at[pl.ds(0, ys - 1)]
    pltpu.make_async_copy(arrived, arrived, proj_recv).wait()
    projected = jnp.concatenate([proj[i] for i in range(ys)], axis=1).astype(jnp.float32)
    residual = stream_ref[...].astype(jnp.float32) + rms_scale(projected, branch_ref[...])
    residual = residual.astype(jnp.bfloat16)
    residuals[...] = residual
    inputs = rms_scale(residual.astype(jnp.float32), pre_ref[...]).astype(jnp.bfloat16)
    piece = D // CHUNKS
    segments = piece // LANES
    for c in range(CHUNKS):
        tokens[c] = inputs[:, c * piece : (c + 1) * piece].reshape(rows, segments, LANES)
    for copy in tables:
        copy.wait()

    def neighbour(i):
        first = lax.rem(place // per + 1 + i // per, 2)
        return first * per + lax.rem(place + lax.rem(i, per), per)

    def exchange(src, dst, send, recv, peer):
        where = side_half * near + peer

        @pl.when(peer != place)
        def _():
            remote(src.at[peer], dst.at[place], send, recv, where_is(where)).start()

        @pl.when(peer == place)
        def _():
            pltpu.make_async_copy(src.at[place], dst.at[place], recv).start()

    def dispatch(t, c, start, stop):
        @pl.loop(start, stop)
        def _(i):
            peer = neighbour(i)
            for r in range(cap):
                source = jnp.clip(sources[t, 0, peer * cap + r], 0, rows - 1)
                outgoing[t, c, peer, r] = far_tokens[c][source] if t else tokens[c, source]
            exchange(outgoing.at[t, c], arrivals.at[t, c], row_send, row_recv.at[t, c], peer)

    def send_tokens():
        for c in range(CHUNKS):
            remote(
                tokens.at[c], far_tokens[c], token_send, token_recv.at[c], where_is(mirror)
            ).start()

    inner = side_half + place // per == 1

    @pl.when(inner)
    def _():
        send_tokens()

    for c in range(CHUNKS):
        dispatch(0, c, 0, per)

    @pl.when(jnp.logical_not(inner))
    def _():
        send_tokens()

    for c in range(CHUNKS):
        dispatch(0, c, per, near)

    def await_rows(t, c):
        pltpu.make_async_copy(arrivals.at[t, c], arrivals.at[t, c], row_recv.at[t, c]).wait()

    def answer(t, c):
        @pl.loop(0, near)
        def _(i):
            exchange(
                results.at[t, c], returned[t][c], back_send, back_recv.at[t, c], neighbour(i)
            )

    def expert_rows(t):
        gate_part, up_part = None, None
        for c in range(CHUNKS):
            await_rows(t, c)
            x = arrivals[t, c].reshape(near * cap, piece)
            cut = slice(c * piece, (c + 1) * piece)
            g = jnp.dot(x, gate_w[cut, :], preferred_element_type=jnp.float32)
            u = jnp.dot(x, up_w[cut, :], preferred_element_type=jnp.float32)
            gate_part = g if c == 0 else gate_part + g
            up_part = u if c == 0 else up_part + u
        hidden = (jax.nn.silu(gate_part) * up_part).astype(jnp.bfloat16)
        for c in range(CHUNKS):
            result = jnp.dot(
                hidden, down_w[:, c * piece : (c + 1) * piece], preferred_element_type=jnp.float32
            )
            results[t, c] = result.astype(jnp.bfloat16).reshape(near, cap, segments, LANES)
            if t == 1:
                answer(t, c)

    def await_sums(t, c):
        pltpu.make_async_copy(returned[t][c], returned[t][c], back_recv.at[t, c]).wait()

    def token_sums(t, c, store, start, stop):
        @pl.loop(start // 8, stop // 8)
        def _(i):
            for k in range(8):
                at = i * 8 + k
                parts = [
                    returned[t][c][
                        jnp.clip(slots[t, j, at], 0, near - 1),
                        jnp.clip(slots[t, TOP + j, at], 0, cap - 1),
                    ].astype(jnp.float32) * shares[t, j, at]
                    for j in range(TOP)
                ]
                store(at, sum(parts))

    for copy in weights:
        copy.wait()
    for c in range(CHUNKS):
        pltpu.make_async_copy(far_tokens[c], far_tokens[c], token_recv.at[c]).wait()
        dispatch(1, c, 0, near)
        if c == CHUNKS // 2 - 1:
            expert_rows(0)
    expert_rows(1)
    for c in range(2):
        answer(0, c)
    for c in range(CHUNKS):
        def store_far(at, value, c=c):
            sums_out[c, at] = value.astype(jnp.bfloat16)

        await_sums(1, c)
        for start in (0, rows // 2):
            some = pl.ds(start, rows // 2)
            token_sums(1, c, store_far, start, start + rows // 2)
            remote(
                sums_out.at[c, some], sums_in.at[c, some], sum_send, sum_recv.at[c],
                where_is(mirror),
            ).start()
        if c < CHUNKS - 2:
            answer(0, c + 2)
    for c in range(CHUNKS):
        def store_own(at, value, c=c):
            combined[c, at] = value

        await_sums(0, c)
        token_sums(0, c, store_own, 0, rows)
    whole = []
    for c in range(CHUNKS):
        pltpu.make_async_copy(sums_in.at[c], sums_in.at[c], sum_recv.at[c]).wait()
        value = combined[c] + sums_in[c].astype(jnp.float32)
        whole.append(value.reshape(rows, piece))
    routed = rms_scale(jnp.concatenate(whole, axis=1), post_ref[...])
    out_ref[...] = (residuals[...].astype(jnp.float32) + routed).astype(jnp.bfloat16)

    for copy in far_copies:
        copy.wait_send()
    pltpu.make_async_copy(tokens, tokens, token_send).wait()
    pltpu.make_async_copy(sums_out, sums_out, sum_send).wait()
    others = pl.ds(0, near - 1)
    for ref, sem in ((outgoing, row_send), (results, back_send)):
        done = ref.at[:, :, others]
        pltpu.make_async_copy(done, done, sem).wait()

    sent = extras.at[pl.ds(0, sp_count - 1)]
    pltpu.make_async_copy(sent, sent, extra_send).wait()
    pltpu.make_async_copy(states_out, states_out, state_send).wait()
    pltpu.make_async_copy(decays_out, decays_out, decay_send).wait()
    w_copy.wait_send()
    pltpu.make_async_copy(crossed, crossed, cross_send).wait()

    @pl.when(pair < pairs - 1)
    def _():
        pltpu.make_async_copy(onward, onward, chain_send).wait()

    for k in range(1, ys):
        pltpu.make_async_copy(own_heads, own_heads, head_send.at[k - 1]).wait()
    pltpu.make_async_copy(proj_out, proj_out, proj_send).wait()


def layer(
    query, key, value, gate, stream, weight, gate_weight, up_weight, down_weight,
    extra, gain, branch_gain, pre_gain, post_gain, chosen, logits,
):
    rows, width = query.shape
    heads = width // KEY_WIDTH
    half = heads // 2
    sp_count, dp_count = lax.axis_size("sp"), lax.axis_size("dp")
    ys = dp_count // 2
    total = sp_count * dp_count
    cols = weight.shape[1]
    cap = max(2, 5 * rows * TOP // (3 * total))
    bf16, f32, i32 = jnp.bfloat16, jnp.float32, jnp.int32
    vmem = pl.BlockSpec(memory_space=pltpu.VMEM)
    anywhere = pl.BlockSpec(memory_space=pl.ANY)
    state = (DV, KEY_WIDTH)
    near = total // 2
    table = (2, 1, -(-near * cap // LANES) * LANES)
    segments = D // CHUNKS // LANES
    units = pltpu.VMEM((2, CHUNKS, near, cap, segments, LANES), bf16)
    unit = pltpu.VMEM((near, cap, segments, LANES), bf16)
    sums = pltpu.VMEM((CHUNKS, rows, segments, LANES), bf16)
    dma = pltpu.SemaphoreType.DMA
    return pl.pallas_call(
        layer_kernel,
        in_specs=[anywhere] * 9 + [vmem] * 7,
        out_specs=vmem,
        out_shape=jax.ShapeDtypeStruct((rows, D), bf16),
        scratch_shapes=[
            pltpu.VMEM((rows, width), bf16),
            pltpu.VMEM((rows, width), bf16),
            pltpu.VMEM(value.shape, bf16),
            pltpu.VMEM((rows, width), bf16),
            pltpu.VMEM((rows, D), bf16),
            pltpu.VMEM((2,) + weight.shape, bf16),
            pltpu.VMEM((sp_count, extra.shape[0], rows), f32),
            pltpu.VMEM((rows, width), f32),
            pltpu.VMEM((rows, width), bf16),
            pltpu.VMEM((rows, width), bf16),
            pltpu.VMEM((rows, width), bf16),
            pltpu.VMEM(value.shape, f32),
            pltpu.VMEM((half,) + state, bf16),
            pltpu.VMEM((2, half) + state, bf16),
            pltpu.VMEM((half, 1, KEY_WIDTH), f32),
            pltpu.VMEM((2, half, 1, KEY_WIDTH), f32),
            pltpu.VMEM((2, half) + state, bf16),
            pltpu.VMEM((half,) + state, bf16),
            pltpu.VMEM((half,) + state, bf16),
            pltpu.VMEM((heads, rows, DV), bf16),
            pltpu.VMEM((ys - 1, heads, rows, DV), bf16),
            pltpu.VMEM((ys - 1, rows, 2 * cols), bf16),
            pltpu.VMEM((ys, rows, 2 * cols), bf16),
            dma((6,)), dma((2,)), dma, dma, dma, dma((half, PARTS)), dma, dma((half,)),
            dma, dma((half, PARTS)), dma, dma((half,)), dma((ys - 1,)), dma((ys - 1, heads)), dma, dma,
            pltpu.VMEM((rows, D), bf16),
            sums, [pltpu.VMEM((rows, segments, LANES), bf16)] * CHUNKS,
            units, units, units, [[unit] * CHUNKS] * 2, sums, sums,
            pltpu.VMEM((CHUNKS, rows, segments, LANES), f32),
            *[pltpu.VMEM(w.shape[1:], bf16) for w in (gate_weight, up_weight, down_weight)],
            pltpu.VMEM((TOP, rows), i32),
            pltpu.VMEM((TOP, rows), f32),
            pltpu.VMEM((2, 2 * TOP, rows), i32),
            pltpu.VMEM(table, i32),
            pltpu.VMEM((2, TOP, rows), f32),
            pltpu.SMEM((2, 2 * TOP, rows), i32),
            pltpu.SMEM(table, i32),
            pltpu.SMEM((2, TOP, rows), f32),
            dma((3,)), dma((3,)), dma((2,)), dma((2,)), dma, dma((CHUNKS,)), dma, dma((2, CHUNKS)),
            dma, dma((2, CHUNKS)), dma, dma((CHUNKS,)),
        ],
        compiler_params=pltpu.CompilerParams(
            collective_id=0, has_side_effects=True, vmem_limit_bytes=60 * 1024 * 1024
        ),
        name="layer",
    )(
        query, key, value, gate, stream, weight, gate_weight, up_weight, down_weight,
        extra, gain.reshape(1, -1), branch_gain.reshape(1, -1), pre_gain.reshape(1, -1),
        post_gain.reshape(1, -1), chosen, logits,
    )


def shards(
    skip_stream_entering,
    mapped_probe_matrix,
    mapped_lookup_matrix,
    mapped_content_matrix,
    retention_preactivation,
    extra_shrinkage,
    attention_group_scale,
    final_projection_matrix,
    blender_branch_scale,
    specialist_prenormal_scale,
    specialist_switch_matrix,
    specialist_expand_matrix,
    specialist_contract_matrix,
    specialist_branch_scale,
    assigned_specialists,
    dispatcher_logits,
):
    out = layer(
        mapped_probe_matrix[0],
        mapped_lookup_matrix[0],
        mapped_content_matrix[0],
        retention_preactivation[0],
        skip_stream_entering[0],
        final_projection_matrix,
        specialist_switch_matrix,
        specialist_expand_matrix,
        specialist_contract_matrix,
        extra_shrinkage[0],
        attention_group_scale,
        blender_branch_scale,
        specialist_prenormal_scale,
        specialist_branch_scale,
        jnp.transpose(assigned_specialists[0]),
        jnp.transpose(dispatcher_logits[0]),
    )
    return out[None]


def solution(mesh):
    return jax.shard_map(
        shards,
        mesh=mesh,
        in_specs=(
            P("dp", "sp", None),
            P("dp", "sp", None),
            P("dp", "sp", None),
            P("dp", "sp", None),
            P("dp", "sp", None),
            P("dp", "sp", None),
            P(),
            P(None, "dp"),
            P(),
            P(),
            P(("sp", "dp"), None, None),
            P(("sp", "dp"), None, None),
            P(("sp", "dp"), None, None),
            P(),
            P("dp", "sp", None),
            P("dp", "sp", None),
        ),
        out_specs=P("dp", "sp", None),
        check_vma=False,
    )
```
